32 devices in a mesh: tp: 8 (over z, x), dp: 4 (over y, core).
Axes of the slice: x: 2, y: 2, z: 4, core: 2. Of those that a mesh axis runs over, the one named last changes fastest.
Arguments:
- tokens: bfloat16 [112, 4096], P('tp', 'dp'), may hold values from -6 to 6
- w_query: bfloat16 [2, 4096, 4096], P(None, 'dp', 'tp'), may hold values from -0.09375 to 0.09375
- w_key: bfloat16 [2, 4096, 4096], P(None, 'dp', 'tp'), may hold values from -0.09375 to 0.09375
- w_value: bfloat16 [2, 4096, 4096], P(None, 'dp', 'tp'), may hold values from -0.09375 to 0.09375
- w_outgate: bfloat16 [2, 4096, 4096], P(None, 'dp', 'tp'), may hold values from -0.09375 to 0.09375
- w_ingate: bfloat16 [2, 4096, 32], P(None, 'dp'), may hold values from -0.09375 to 0.09375
- w_forget: bfloat16 [2, 4096, 32], P(None, 'dp'), may hold values from -0.09375 to 0.09375
- forget_bias: float32 [2, 32], P(None, 'tp'), may hold values from -2 to 3
- head_gain: float32 [2, 32, 128], P(None, 'tp'), may hold values from 0.1 to 1.9
- w_proj: bfloat16 [2, 4096, 4096], P(None, 'tp', 'dp'), may hold values from -0.09375 to 0.09375
- mem_matrix: float32 [2, 112, 32, 128, 128], P(None, 'dp', 'tp'), may hold values from -0.8 to 0.8
- mem_norm: float32 [2, 112, 32, 128], P(None, 'dp', 'tp'), may hold values from -1.2 to 1.2
- mem_max: float32 [2, 112, 32], P(None, 'dp', 'tp'), may hold values from -4 to 4
Outputs:
- result: bfloat16 [112, 4096], P('tp', 'dp')
- new_matrix: float32 [2, 112, 32, 128, 128], P(None, 'dp', 'tp')
- new_norm: float32 [2, 112, 32, 128], P(None, 'dp', 'tp')
- new_max: float32 [2, 112, 32], P(None, 'dp', 'tp')
The draws below stay inside these ranges and needn't reach their ends.
All inputs are finite; a program needn't handle non-finite values.
Results may differ from the reference program's by a relative error of at most 0.017.
Values may be sent and summed in bfloat16 or wider, within the bound.
No kernel may reach another device: no remote copies, remote signals or barrier semaphores. Data moves between devices by JAX's collectives and lax.ppermute only.
A program may use at most 128 MiB of HBM per device.

```python
import jax
import jax.numpy as jnp
from jax import lax

D = 4096
HEADS = 32
HEAD = 128
BLOCKS = 2
BATCH = 112


def level_of(key, shape, pieces, low, largest):
    def one(position, blocks):
        draws = jax.random.uniform(jax.random.fold_in(jax.random.fold_in(key, 6), position), (blocks,), jnp.float32, low / len(pieces), largest / len(pieces))
        return jnp.repeat(jnp.exp(draws), shape[position] // blocks).reshape((-1,) + (1,) * (len(shape) - position - 1))

    loudness = one(*pieces[0])
    for cut in pieces[1:]:
        loudness = loudness * one(*cut)
    return loudness


def gaussian(stream_key, shape, deviation, limit, cuts=(), held_as=jnp.bfloat16):
    level = level_of(stream_key, shape, cuts, -0.22, 0.18) if cuts else 1.0
    array = jax.random.normal(stream_key, shape, jnp.float32) * deviation * level
    return jnp.minimum(jnp.maximum(array, -limit), limit).astype(held_as)


def setup_inputs(seed: int = 0) -> dict:
    keys = jax.random.split(jax.random.key(seed), 14)
    return {
        "tokens": gaussian(keys[0], (BATCH, D), 1.0, 6.0, ((0, 8), (1, 4))),
        "w_query": gaussian(keys[1], (BLOCKS, D, D), D ** -0.5, 0.09375, ((1, 4), (2, 8))),
        "w_key": gaussian(keys[2], (BLOCKS, D, D), D ** -0.5, 0.09375, ((1, 4), (2, 8))),
        "w_value": gaussian(keys[3], (BLOCKS, D, D), D ** -0.5, 0.09375, ((1, 4), (2, 8))),
        "w_outgate": gaussian(keys[4], (BLOCKS, D, D), D ** -0.5, 0.09375, ((1, 4), (2, 8))),
        "w_ingate": gaussian(keys[5], (BLOCKS, D, HEADS), D ** -0.5, 0.09375, ((1, 4),)),
        "w_forget": gaussian(keys[6], (BLOCKS, D, HEADS), D ** -0.5, 0.09375, ((1, 4),)),
        "forget_bias": jnp.clip(-2.0 + 5.0 * jax.random.uniform(keys[7], (BLOCKS, HEADS), jnp.float32) ** level_of(keys[7], (BLOCKS, HEADS), ((1, 8),), -0.2, 0.2), -2.0, 3.0),
        "head_gain": jnp.clip(1.0 + 0.18 * jax.random.normal(keys[8], (BLOCKS, HEADS, HEAD), jnp.float32), 0.1, 1.9),
        "w_proj": gaussian(keys[9], (BLOCKS, D, D), D ** -0.5, 0.09375, ((1, 8), (2, 4))),
        "mem_matrix": gaussian(keys[10], (BLOCKS, BATCH, HEADS, HEAD, HEAD), 0.1, 0.8, ((1, 4), (2, 8)), jnp.float32),
        "mem_norm": gaussian(keys[11], (BLOCKS, BATCH, HEADS, HEAD), 0.15, 1.2, ((1, 4), (2, 8)), jnp.float32),
        "mem_max": gaussian(keys[12], (BLOCKS, BATCH, HEADS), 1.0, 4.0, ((1, 4), (2, 8)), jnp.float32),
    }


norm_eps = 1e-06
head_eps = 1e-05

def full_sum(x_rows, weight):
    return jnp.dot(x_rows, weight, preferred_element_type=jnp.float32)

def cell_update(queries, key_vecs, values, log_in, log_forget, matrix, normvec, maxval):
    max_next = jnp.maximum(log_forget + maxval, log_in)
    decays = jnp.exp(log_forget + maxval - max_next)
    weight_in = jnp.exp(log_in - max_next)
    matrix_new = decays[..., None, None] * matrix + weight_in[..., None, None] * key_vecs[..., :, None] * values[..., None, :]
    norm_new = decays[..., None] * normvec + weight_in[..., None] * key_vecs
    numerator = jnp.einsum('bhd,bhde->bhe', queries, matrix_new, precision=lax.Precision.HIGHEST)
    denominator = jnp.maximum(jnp.abs(lax.optimization_barrier(jnp.sum(queries * norm_new, axis=-1))), 1.0)
    return (numerator / denominator[..., None], matrix_new, norm_new, max_next)

def head_norm(readout, gain, outgate):
    average = lax.optimization_barrier(jnp.mean(readout, axis=-1, keepdims=True))
    variance = lax.optimization_barrier(jnp.mean(jnp.square(readout - average), axis=-1, keepdims=True))
    normed = (readout - average) * lax.rsqrt(variance + head_eps) * gain
    return normed * jax.nn.sigmoid(outgate)

def mix_block(x_rows, weights, states):
    w_query, w_key, w_value, w_outgate, w_ingate, w_forget, bias, gain, w_proj = weights
    matrix, normvec, maxval = states
    row_count, features = x_rows.shape
    squares = lax.optimization_barrier(jnp.sum(jnp.square(x_rows.astype(jnp.float32)), axis=1))
    inv_scale = lax.rsqrt(squares / features + norm_eps)[:, None]
    head_shape = (row_count, HEADS, HEAD)
    queries = (full_sum(x_rows, w_query) * inv_scale).reshape(head_shape)
    key_vecs = (full_sum(x_rows, w_key) * inv_scale * HEAD ** (-0.5)).reshape(head_shape)
    values = (full_sum(x_rows, w_value) * inv_scale).reshape(head_shape)
    outgate = (full_sum(x_rows, w_outgate) * inv_scale).reshape(head_shape)
    log_in = full_sum(x_rows, w_ingate) * inv_scale
    log_forget = jax.nn.log_sigmoid(full_sum(x_rows, w_forget) * inv_scale + bias[None, :])
    readout, matrix_new, norm_new, max_next = cell_update(queries, key_vecs, values, log_in, log_forget, matrix, normvec, maxval)
    hidden = head_norm(readout, gain[None], outgate).reshape(row_count, -1).astype(jnp.bfloat16)
    mixed_out = jnp.dot(hidden, w_proj, preferred_element_type=jnp.float32).astype(jnp.bfloat16)
    return (mixed_out, matrix_new, norm_new, max_next)

def reference(tokens, w_query, w_key, w_value, w_outgate, w_ingate, w_forget, forget_bias, head_gain, w_proj, mem_matrix, mem_norm, mem_max):
    current = tokens
    matrix_list, norm_list, max_list = ([], [], [])
    for block_id in range(BLOCKS):
        weights = (w_query[block_id], w_key[block_id], w_value[block_id], w_outgate[block_id], w_ingate[block_id], w_forget[block_id], forget_bias[block_id], head_gain[block_id], w_proj[block_id])
        current, matrix_out, norm_out, max_out = mix_block(current, weights, (mem_matrix[block_id], mem_norm[block_id], mem_max[block_id]))
        matrix_list.append(matrix_out)
        norm_list.append(norm_out)
        max_list.append(max_out)
    return (current, jnp.stack(matrix_list), jnp.stack(norm_list), jnp.stack(max_list))
```

```python
import functools

import jax
import jax.numpy as jnp
from jax import lax
from jax.experimental import pallas as pl
from jax.experimental.pallas import tpu as pltpu
from jax.sharding import PartitionSpec as P

norm_eps = 1e-06
head_eps = 1e-05
PAD = 16
LANES = 128
UP = 12.0
TINY = 1e-30
OUT_UP = 16.0
F32 = jnp.float32
BF16 = jnp.bfloat16


def lane_roll(x, amount):
    return pltpu.roll(x, amount % x.shape[-1], 1)


def project_kernel(block, heads_all, meta, x, wq, wk, wv, wo, wi, wf, own, *rest):
    sends, (x_rel, gates, wide_w, gate_w, sems) = rest[:-5], rest[-5:]
    copies = [
        pltpu.make_async_copy(source.at[block], target.at[i], sems.at[n])
        for n, (source, target, i) in enumerate(
            [(wi, gate_w, 0), (wf, gate_w, 1), (wq, wide_w, 0), (wk, wide_w, 1), (wv, wide_w, 2), (wo, wide_w, 3)]
        )
    ]
    for copy in copies:
        copy.start()
    slots = len(sends) + 1
    rows = x.shape[0] // slots
    me = meta[0]
    first_head = meta[1]
    for slot in range(slots):
        start = pl.multiple_of((me ^ slot) * rows, rows)
        x_rel[slot * rows : (slot + 1) * rows, :] = x[pl.ds(start, rows), :]
    xs = x_rel[...]
    cols = wq.shape[2]

    wide = xs.astype(F32)
    squares = jnp.sum(wide * wide, axis=1, keepdims=True)
    power = jnp.floor(0.5 * jnp.log2(squares + TINY))
    scale = jnp.exp2(UP - power)

    def emit(value, offset):
        width = value.shape[1]
        for slot, send in enumerate((own,) + tuple(sends)):
            send[:, offset : offset + width] = value[slot * rows : (slot + 1) * rows]

    gates[...] = jnp.zeros(gates.shape, F32)
    for index in range(2):
        copies[index].wait()
        value = jnp.dot(xs, gate_w[index], preferred_element_type=F32)
        gates[:, index * heads_all : (index + 1) * heads_all] = value
    lane = lax.broadcasted_iota(jnp.int32, gates.shape, 1)
    mine = pltpu.roll(gates[...], (LANES - first_head) % LANES, 1)
    mine = mine * scale
    mine = jnp.where(lane == heads_all - 1, squares * jnp.exp2(-2.0 * power), mine)
    mine = jnp.where(lane == heads_all - 2, power, mine)
    low = mine - mine.astype(BF16).astype(F32)
    emit(jnp.where(lane < LANES // 2, mine, pltpu.roll(low, LANES // 2, 1)), 4 * cols)
    for index in range(4):
        copies[2 + index].wait()
        emit(jnp.dot(xs, wide_w[index], preferred_element_type=F32) * scale, index * cols)


def project(block, meta, x, wq, wk, wv, wo, wi, wf, slots):
    rows = x.shape[0] // slots
    heads_all = wi.shape[2]
    width = 4 * wq.shape[2] + LANES
    whole = pl.BlockSpec(memory_space=pltpu.VMEM)

    return pl.pallas_call(
        functools.partial(project_kernel, block, heads_all),
        in_specs=[pl.BlockSpec(memory_space=pltpu.SMEM), whole] + [pl.BlockSpec(memory_space=pltpu.HBM)] * 6,
        out_specs=[whole] * slots,
        out_shape=[jax.ShapeDtypeStruct((rows, width), F32)] * slots,
        scratch_shapes=[
            pltpu.VMEM(x.shape, BF16),
            pltpu.VMEM((x.shape[0], LANES), F32),
            pltpu.VMEM((4,) + wq.shape[1:], BF16),
            pltpu.VMEM((2,) + wi.shape[1:], BF16),
            pltpu.SemaphoreType.DMA((6,)),
        ],
        compiler_params=pltpu.CompilerParams(vmem_limit_bytes=32 << 20),
        cost_estimate=pl.CostEstimate(
            flops=2 * x.shape[0] * x.shape[1] * width, bytes_accessed=5 << 20, transcendentals=0
        ),
        name="project",
    )(meta, x, wq, wk, wv, wo, wi, wf)


def spread(pairs, real):
    return [(slice(i * PAD, i * PAD + real), slice(i * real, (i + 1) * real)) for i in range(pairs)]


def cell_kernel(features, heads_all, peers, *refs):
    own = refs[0]
    parts = refs[1 : 1 + peers]
    bias, gain, norm, maxval, matrix = refs[1 + peers : 6 + peers]
    rest = refs[6 + peers :]
    if len(rest) > 13:
        rest = rest[2:]
    (hidden, norm_out, max_out, kw_out, v_out, dec_out) = rest[:6]
    (q_s, o_s, qw_s, n_s, nn_s, mp_s, part_s) = rest[6:]
    head = pl.program_id(0)
    heads = norm.shape[2]
    rows, real = own.shape[0], norm.shape[1]
    pairs = rows // PAD
    moves = spread(pairs, real // pairs)
    cols = heads * LANES

    @pl.when(head == 0)
    def _():
        scales, packed, squares = [], 0.0, 0.0
        for part in (own,) + tuple(parts):
            tile = part[:, 4 * cols :]
            tile = tile + lane_roll(tile, LANES // 2)
            power = tile[:, heads_all - 2 : heads_all - 1]
            scales.append(jnp.exp2(power - UP))
            packed = packed + tile * scales[-1]
            squares = squares + tile[:, heads_all - 1 : heads_all] * jnp.exp2(2.0 * power)

        def total(start, width):
            value = 0.0
            for part, scale in zip((own,) + tuple(parts), scales):
                value = value + part[:, start : start + width] * scale
            return value

        inv = lax.rsqrt(squares / features + norm_eps)
        log_in = packed[:, :heads] * inv
        raw = packed[:, heads_all : heads_all + heads] * inv + bias[0]
        log_forget = jnp.minimum(raw, 0.0) - jnp.log1p(jnp.exp(-jnp.abs(raw)))
        mp_s[...] = jnp.zeros(mp_s.shape, F32)
        for padded, plain in moves:
            mp_s[padded, :] = maxval[0, plain, :]
        carried = log_forget + mp_s[...]
        new_max = jnp.maximum(carried, log_in)
        decays = jnp.exp(carried - new_max)
        weight_in = jnp.exp(log_in - new_max)
        for padded, plain in moves:
            max_out[0, plain, :] = new_max[padded]
        n_s[...] = jnp.zeros(n_s.shape, F32)
        for h in range(heads):
            for padded, plain in moves:
                n_s[h, padded, :] = norm[0, plain, h, :]
            at = h * LANES
            q = total(at, LANES) * inv
            k = total(cols + at, LANES) * (inv * LANES ** (-0.5))
            q_s[h] = q
            v_out[h] = total(2 * cols + at, LANES) * inv
            o_s[h] = total(3 * cols + at, LANES) * inv
            dec = jnp.broadcast_to(decays[:, h : h + 1], (rows, LANES))
            dec_out[h] = dec
            kw = k * weight_in[:, h : h + 1]
            kw_out[h] = kw
            nn = dec * n_s[h] + kw
            nn_s[h] = nn
            for padded, plain in moves:
                norm_out[0, plain, h, :] = nn[padded]
        part_s[...] = jnp.zeros(part_s.shape, F32)

    q = q_s[head]
    q_t = q.T
    for padded, plain in moves:
        for row, seq in zip(range(rows)[padded], range(real)[plain]):
            column = jnp.broadcast_to(q_t[:, row : row + 1], (LANES, LANES))
            product = matrix[0, seq, 0] * column
            part_s[row * 8 : row * 8 + 8, :] = jnp.sum(product.reshape(LANES // 8, 8, LANES), axis=0)
    carried = part_s[pl.ds(0, rows, stride=8), :]
    for j in range(1, 8):
        carried = carried + part_s[pl.ds(j, rows, stride=8), :]
    kw = kw_out[head]
    scores = jnp.sum(q * kw, axis=1, keepdims=True)
    denominator = jnp.maximum(jnp.abs(jnp.sum(q * nn_s[head], axis=1, keepdims=True)), 1.0)
    readout = (dec_out[head] * carried + scores * v_out[head]) / denominator
    average = jnp.mean(readout, axis=1, keepdims=True)
    centred = readout - average
    variance = jnp.mean(centred * centred, axis=1, keepdims=True)
    normed = centred * lax.rsqrt(variance + head_eps) * gain[0, pl.ds(head, 1), :]
    hidden[...] = (normed * jax.nn.sigmoid(o_s[head])).astype(BF16)


def cell(block, own, parts, bias, gain, norm, maxval, matrix, heads_all, features, filled):
    rows = own.shape[0]
    blocks, real, heads, _ = norm.shape
    full = lambda a: pl.BlockSpec(a.shape, lambda h: (0,) * a.ndim)
    at = lambda a: pl.BlockSpec((1,) + a.shape[1:], lambda h: (block,) + (0,) * (a.ndim - 1))
    gates = jax.ShapeDtypeStruct((heads, rows, LANES), F32)
    aliased = [] if filled is None else list(filled)
    base = 6 + len(parts)
    bias = bias[:, None]
    return pl.pallas_call(
        functools.partial(cell_kernel, features, heads_all, len(parts)),
        grid=(heads,),
        in_specs=[full(own)]
        + [full(p) for p in parts]
        + [at(bias), at(gain), at(norm), at(maxval)]
        + [pl.BlockSpec((1, real, 1, LANES, LANES), lambda h: (block, 0, h, 0, 0))]
        + [pl.BlockSpec(memory_space=pl.ANY)] * len(aliased),
        out_specs=[
            pl.BlockSpec((rows, LANES), lambda h: (0, h)),
            at(norm),
            at(maxval),
            full(gates),
            full(gates),
            full(gates),
        ],
        out_shape=[
            jax.ShapeDtypeStruct((rows, heads * LANES), BF16),
            jax.ShapeDtypeStruct(norm.shape, F32),
            jax.ShapeDtypeStruct(maxval.shape, F32),
            gates,
            gates,
            gates,
        ],
        input_output_aliases={base: 1, base + 1: 2} if aliased else {},
        scratch_shapes=[pltpu.VMEM((heads, rows, LANES), F32)] * 5
        + [pltpu.VMEM((rows, heads), F32), pltpu.VMEM((rows * 8, LANES), F32)],
        compiler_params=pltpu.CompilerParams(vmem_limit_bytes=32 << 20),
        cost_estimate=pl.CostEstimate(
            flops=4 * real * heads * LANES * LANES,
            bytes_accessed=4 * real * heads * LANES * LANES,
            transcendentals=0,
        ),
        name="cell",
    )(own, *parts, bias, gain, norm, maxval, matrix, *aliased)


def update_kernel(kw, v, dec, matrix, *rest):
    out = rest[-1]
    head = pl.program_id(0)
    rows, real = kw.shape[1], matrix.shape[1]
    pairs = rows // PAD
    kw_t = kw[head].T
    for padded, plain in spread(pairs, real // pairs):
        for row, seq in zip(range(rows)[padded], range(real)[plain]):
            column = jnp.broadcast_to(kw_t[:, row : row + 1], (LANES, LANES))
            decay = dec[head, row : row + 1, :]
            out[0, seq, 0] = decay * matrix[0, seq, 0] + column * v[head, row : row + 1, :]


def update(block, kw, v, dec, matrix, filled):
    _, real, heads = matrix.shape[:3]
    full = lambda a: pl.BlockSpec(a.shape, lambda h: (0,) * a.ndim)
    one = pl.BlockSpec((1, real, 1, LANES, LANES), lambda h: (block, 0, h, 0, 0))
    aliased = [] if filled is None else [filled]
    return pl.pallas_call(
        update_kernel,
        grid=(heads,),
        in_specs=[full(kw), full(v), full(dec), one] + [pl.BlockSpec(memory_space=pl.ANY)] * len(aliased),
        out_specs=one,
        out_shape=jax.ShapeDtypeStruct(matrix.shape, F32),
        input_output_aliases={4: 0} if aliased else {},
        compiler_params=pltpu.CompilerParams(vmem_limit_bytes=32 << 20),
        cost_estimate=pl.CostEstimate(
            flops=4 * real * heads * LANES * LANES,
            bytes_accessed=8 * real * heads * LANES * LANES,
            transcendentals=0,
        ),
        name="update",
    )(kw, v, dec, matrix, *aliased)


def output_kernel(meta, w, *refs):
    parts, out = refs[:-1], refs[-1]
    rows = parts[0].shape[0]
    me = meta[0]
    value = jnp.dot(
        jnp.concatenate([part[...] for part in parts], axis=0), w[0], preferred_element_type=F32
    )
    value = value * OUT_UP
    for slot in range(len(parts)):
        start = pl.multiple_of((me ^ slot) * rows, rows)
        out[pl.ds(start, rows), :] = value[slot * rows : (slot + 1) * rows]


def output(block, meta, w, parts):
    rows = parts[0].shape[0]
    whole = pl.BlockSpec(memory_space=pltpu.VMEM)
    return pl.pallas_call(
        output_kernel,
        in_specs=[
            pl.BlockSpec(memory_space=pltpu.SMEM),
            pl.BlockSpec((1,) + w.shape[1:], lambda i: (block, 0, 0)),
        ]
        + [whole] * len(parts),
        grid=(1,),
        out_specs=whole,
        out_shape=jax.ShapeDtypeStruct((rows * len(parts), w.shape[2]), F32),
        compiler_params=pltpu.CompilerParams(vmem_limit_bytes=16 << 20),
        cost_estimate=pl.CostEstimate(
            flops=2 * rows * len(parts) * w.shape[1] * w.shape[2], bytes_accessed=1 << 20, transcendentals=0
        ),
        name="output",
    )(meta, w, *parts)


def swap(x, axis, size, bit):
    return lax.ppermute(x, axis, [(i, i ^ bit) for i in range(size)])


def on_device(
    tokens,
    w_query,
    w_key,
    w_value,
    w_outgate,
    w_ingate,
    w_forget,
    forget_bias,
    head_gain,
    w_proj,
    mem_matrix,
    mem_norm,
    mem_max,
):
    tp, dp = lax.axis_size("tp"), lax.axis_size("dp")
    real = tokens.shape[0]
    features = tokens.shape[1]
    heads = forget_bias.shape[1]
    heads_all = w_ingate.shape[2]
    assert dp & (dp - 1) == 0 and tp % dp == 0 and real <= PAD and 2 * heads_all <= LANES // 2
    meta = jnp.stack([lax.axis_index("dp"), lax.axis_index("tp") * heads]).astype(jnp.int32)

    def gather(rows):
        spread_rows = jnp.broadcast_to(rows[None], (tp,) + rows.shape)
        return lax.all_to_all(spread_rows, "tp", 0, 0).reshape(tp * PAD, features)

    current = gather(jnp.pad(tokens, ((0, PAD - real), (0, 0))))
    blocks = w_query.shape[0]
    filled, matrix_out = None, None
    for block in range(blocks):
        own, *sends = project(
            block, meta, current, w_query, w_key, w_value, w_outgate, w_ingate, w_forget, dp
        )
        parts = [
            swap(part.astype(jnp.float16), "dp", dp, slot).astype(F32) for slot, part in enumerate(sends, 1)
        ]
        hidden, norm_out, max_out, kw, v, dec = cell(
            block, own, parts, forget_bias, head_gain, mem_norm, mem_max, mem_matrix,
            heads_all, features * dp, filled,
        )
        filled = (norm_out, max_out)
        gathered = [hidden] + [swap(hidden, "dp", dp, slot) for slot in range(1, dp)]
        matrix_out = update(block, kw, v, dec, mem_matrix, matrix_out)
        partial = output(block, meta, w_proj, gathered).reshape(tp, PAD, features)
        summed = lax.all_to_all(partial.astype(jnp.float16), "tp", 0, 0)
        summed = (jnp.sum(summed.astype(F32), axis=0) * (1.0 / OUT_UP)).astype(BF16)
        if block + 1 < blocks:
            current = gather(summed)
    return (summed[:real], matrix_out, *filled)


def solution(mesh):
    in_specs = (
        P("tp", "dp"),
        P(None, "dp", "tp"),
        P(None, "dp", "tp"),
        P(None, "dp", "tp"),
        P(None, "dp", "tp"),
        P(None, "dp", None),
        P(None, "dp", None),
        P(None, "tp"),
        P(None, "tp", None),
        P(None, "tp", "dp"),
        P(None, "dp", "tp", None, None),
        P(None, "dp", "tp", None),
        P(None, "dp", "tp"),
    )
    out_specs = (
        P("tp", "dp"),
        P(None, "dp", "tp", None, None),
        P(None, "dp", "tp", None),
        P(None, "dp", "tp"),
    )
    return jax.shard_map(
        on_device, mesh=mesh, in_specs=in_specs, out_specs=out_specs, check_vma=False
    )
```

```python
import functools

import jax
import jax.numpy as jnp
from jax import lax
from jax.experimental import pallas as pl
from jax.experimental.pallas import tpu as pltpu
from jax.sharding import PartitionSpec as P

norm_eps = 1e-06
head_eps = 1e-05
ROWS = 32
PAD = 16
LANES = 128
UP = 12.0
TINY = 1e-30
OUT_UP = 16.0
F32 = jnp.float32
BF16 = jnp.bfloat16


def in_hbm(x):
    return pltpu.with_memory_space_constraint(x, pltpu.HBM)


def in_vmem(x):
    return pltpu.with_memory_space_constraint(x, pltpu.VMEM)


def lane_roll(x, amount):
    return pltpu.roll(x, amount % x.shape[-1], 1)


def fetch_kernel(steps, count, *refs):
    sources, targets, sems = refs[:count], refs[-1 - steps[1] : -1], refs[-1]
    copies = []
    for source, part, target, place in steps[0]:
        from_ref = sources[source] if part is None else sources[source].at[part]
        to_ref = targets[target] if place is None else targets[target].at[place]
        copies.append(pltpu.make_async_copy(from_ref, to_ref, sems.at[len(copies)]))
    for copy in copies:
        copy.start()
    if steps[2]:
        ones = targets[-1]
        for block in range(ones.shape[1] // LANES):
            row = lax.broadcasted_iota(jnp.int32, (LANES, LANES), 0)
            here = (row % ROWS == block) & (row < 3 * ROWS)
            ones[:, block * LANES : (block + 1) * LANES] = jnp.where(here, 1.0, 0.0).astype(BF16)
    for copy in copies:
        copy.wait()


def fetch(arrays, steps, shapes, with_ones=False, after=()):
    shapes = list(shapes)
    if with_ones:
        shapes.append(((LANES, ROWS * LANES), BF16))
    total = sum(a.size * a.dtype.itemsize for a in arrays)
    return pl.pallas_call(
        functools.partial(fetch_kernel, (steps, len(shapes), with_ones), len(arrays)),
        in_specs=[pl.BlockSpec(memory_space=pltpu.HBM)] * len(arrays)
        + [pl.BlockSpec(memory_space=pl.ANY)] * len(after),
        out_specs=[pl.BlockSpec(memory_space=pltpu.VMEM)] * len(shapes),
        out_shape=[pltpu.VMEM(shape, dtype) for shape, dtype in shapes],
        scratch_shapes=[pltpu.SemaphoreType.DMA((len(steps),))],
        compiler_params=pltpu.CompilerParams(vmem_limit_bytes=8 << 20),
        cost_estimate=pl.CostEstimate(flops=total, bytes_accessed=total, transcendentals=0),
        name="fetch",
    )(*map(in_hbm, arrays), *after)


def begin_kernel(tokens, *refs):
    count = (len(refs) - 2) // 2
    sources, (copied, *targets), sems = refs[:count], refs[count:-1], refs[-1]
    moves = [(tokens, copied.at[i]) for i in range(copied.shape[0])]
    moves += [(source.at[:1], target) for source, target in zip(sources, targets)]
    copies = [
        pltpu.make_async_copy(source, target, sems.at[i]) for i, (source, target) in enumerate(moves)
    ]
    for copy in copies:
        copy.start()
    for copy in copies:
        copy.wait()


def begin(tokens, weights, copies):
    shapes = [((copies,) + tokens.shape, BF16)] + [((1,) + w.shape[1:], BF16) for w in weights]
    whole = pl.BlockSpec(memory_space=pltpu.VMEM)
    return pl.pallas_call(
        begin_kernel,
        in_specs=[pl.BlockSpec(memory_space=pltpu.HBM)] * (1 + len(weights)),
        out_specs=[whole] * len(shapes),
        out_shape=[pltpu.VMEM(shape, dtype) for shape, dtype in shapes],
        scratch_shapes=[pltpu.SemaphoreType.DMA((copies + len(weights),))],
        compiler_params=pltpu.CompilerParams(vmem_limit_bytes=8 << 20),
        name="begin",
    )(*map(in_hbm, (tokens,) + weights))


def project_kernel(block, heads_all, meta, x, wq, wk, wv, wo, wi, wf, own, *rest):
    sends, (x_rel, gates) = rest[:-2], rest[-2:]
    slots = len(sends) + 1
    rows = x_rel.shape[0] // slots
    me = meta[0]
    first_head = meta[1]
    pairs, real = rows // PAD, x.shape[1]
    if real < PAD:
        x_rel[...] = jnp.zeros(x_rel.shape, BF16)
    for slot in range(slots):
        for i in range(pairs):
            at = slot * rows + i * PAD
            x_rel[at : at + real, :] = x[(me ^ slot) * pairs + i]
    xs = x_rel[...]
    cols = wq.shape[2]

    wide = xs.astype(F32)
    squares = jnp.sum(wide * wide, axis=1, keepdims=True)
    power = jnp.floor(0.5 * jnp.log2(squares + TINY))
    scale = jnp.exp2(UP - power)

    def emit(value, offset):
        width = value.shape[1]
        for slot, send in enumerate((own,) + tuple(sends)):
            send[:, offset : offset + width] = value[slot * rows : (slot + 1) * rows]

    for index, weight in enumerate((wq, wk, wv, wo)):
        emit(jnp.dot(xs, weight[block], preferred_element_type=F32) * scale, index * cols)
    gates[...] = jnp.zeros(gates.shape, F32)
    for index, weight in enumerate((wi, wf)):
        value = lax.dot_general(xs, weight[block], (((1,), (1,)), ((), ())), preferred_element_type=F32)
        gates[:, index * heads_all : (index + 1) * heads_all] = value
    lane = lax.broadcasted_iota(jnp.int32, gates.shape, 1)
    mine = pltpu.roll(gates[...], (LANES - first_head) % LANES, 1)
    mine = mine * scale
    mine = jnp.where(lane == heads_all - 1, squares * jnp.exp2(-2.0 * power), mine)
    mine = jnp.where(lane == heads_all - 2, power, mine)
    low = mine - mine.astype(BF16).astype(F32)
    emit(jnp.where(lane < LANES // 2, mine, pltpu.roll(low, LANES // 2, 1)), 4 * cols)


def project(block, meta, x, weights, slots):
    all_rows, features = x.shape[0] * PAD, x.shape[2]
    rows = all_rows // slots
    heads_all = weights[-1].shape[1]
    width = 4 * weights[0].shape[2] + LANES
    whole = pl.BlockSpec(memory_space=pltpu.VMEM)
    return pl.pallas_call(
        functools.partial(project_kernel, block, heads_all),
        in_specs=[pl.BlockSpec(memory_space=pltpu.SMEM)] + [whole] * 7,
        out_specs=[whole] * slots,
        out_shape=[jax.ShapeDtypeStruct((rows, width), F32)] * slots,
        scratch_shapes=[pltpu.VMEM((all_rows, features), BF16), pltpu.VMEM((all_rows, LANES), F32)],
        compiler_params=pltpu.CompilerParams(vmem_limit_bytes=8 << 20),
        cost_estimate=pl.CostEstimate(
            flops=2 * all_rows * features * width, bytes_accessed=1 << 20, transcendentals=0
        ),
        name="project",
    )(meta, x, *map(in_vmem, weights))


def spread(pairs, real):
    return [(slice(i * PAD, i * PAD + real), slice(i * real, (i + 1) * real)) for i in range(pairs)]


def twos(moves):
    runs = []
    for padded, plain in moves:
        length = plain.stop - plain.start
        for j in range(0, length, 2):
            runs.append((padded.start + j, plain.start + j, min(2, length - j)))
    return runs


def pieces(x):
    high = x.astype(BF16).astype(F32)
    return high, x - high


def columns(*parts):
    parts = list(parts)
    rest = LANES - sum(part.shape[0] for part in parts)
    if rest:
        parts.append(jnp.zeros((rest, LANES), F32))
    return jnp.concatenate(parts, axis=0).T.astype(BF16)


def cell_kernel(block, features, heads_all, peers, before, *refs):
    own = refs[0]
    parts = refs[1 : 1 + peers]
    bias, gain, norm, maxval, matrix, ones = refs[1 + peers : 7 + peers]
    earlier = refs[7 + peers : 7 + peers + 2 * before]
    (hidden, norm_out, max_out, kw_out, v_out, dec_out, mp_s, part_s, wide_s, tall_s) = refs[-10:]
    heads = matrix.shape[1]
    rows, real = own.shape[0], matrix.shape[0]
    pairs = rows // PAD
    moves = spread(pairs, real // pairs)
    cols = heads * LANES

    for i in range(before):
        norm_out[i] = earlier[2 * i][0]
        max_out[i] = earlier[2 * i + 1][0]
    norm_out, max_out = norm_out.at[before], max_out.at[before]

    scales, packed, squares = [], 0.0, 0.0
    for part in (own,) + tuple(parts):
        tile = part[:, 4 * cols :]
        tile = tile + lane_roll(tile, LANES // 2)
        power = tile[:, heads_all - 2 : heads_all - 1]
        scales.append(jnp.exp2(power - UP))
        packed = packed + tile * scales[-1]
        squares = squares + tile[:, heads_all - 1 : heads_all] * jnp.exp2(2.0 * power)

    def total(start, width):
        value = 0.0
        for part, scale in zip((own,) + tuple(parts), scales):
            value = value + part[:, start : start + width] * scale
        return value

    inv = lax.rsqrt(squares / features + norm_eps)
    log_in = packed[:, :heads] * inv
    raw = packed[:, heads_all : heads_all + heads] * inv + bias[block : block + 1, :]
    log_forget = jnp.minimum(raw, 0.0) - jnp.log1p(jnp.exp(-jnp.abs(raw)))
    mp_s[...] = jnp.zeros(mp_s.shape, F32)
    tall_s[...] = jnp.zeros(tall_s.shape, F32)
    wide_s[...] = jnp.zeros(wide_s.shape, F32)
    wide_s[:heads, :real] = maxval[block]
    tall = wide_s[...].T
    for padded, plain in moves:
        mp_s[padded, :] = tall[plain, :heads]
    carried = log_forget + mp_s[...]
    new_max = jnp.maximum(carried, log_in)
    decays = jnp.exp(carried - new_max)
    weight_in = jnp.exp(log_in - new_max)
    for padded, plain in moves:
        tall_s[plain, :heads] = new_max[padded]
    max_out[...] = tall_s[...].T[:heads, :real]
    part_s[...] = jnp.zeros(part_s.shape, F32)
    for h in range(heads):
        at = h * LANES
        q = total(at, LANES) * inv
        high, rest = pieces(q)
        middle, low = pieces(rest)
        q_t = columns(high, middle, low)
        for row, seq, count in twos(moves):
            spread_q = jnp.dot(
                q_t, ones[:, row * LANES : (row + count) * LANES], preferred_element_type=F32
            )
            for i in range(count):
                product = matrix[seq + i, h] * spread_q[:, i * LANES : (i + 1) * LANES]
                part_s[h, (row + i) * 8 : (row + i) * 8 + 8, :] = jnp.sum(
                    product.reshape(LANES // 8, 8, LANES), axis=0
                )
        v = total(2 * cols + at, LANES) * inv
        v_out[h] = v
        dec = jnp.broadcast_to(decays[:, h : h + 1], (rows, LANES))
        dec_out[h] = dec
        kw = total(cols + at, LANES) * (inv * LANES ** (-0.5)) * weight_in[:, h : h + 1]
        kw_out[h] = kw
        for padded, plain in moves:
            nn = dec[padded] * norm[block, plain, h, :] + kw[padded]
            norm_out[plain, h, :] = nn
            mp_s[padded, h : h + 1] = jnp.sum(q[padded] * nn, axis=1, keepdims=True)
        denominator = jnp.maximum(jnp.abs(mp_s[:, h : h + 1]), 1.0)
        mixed = part_s[h, pl.ds(0, rows, stride=8), :]
        for j in range(1, 8):
            mixed = mixed + part_s[h, pl.ds(j, rows, stride=8), :]
        scores = jnp.sum(q * kw, axis=1, keepdims=True)
        readout = (dec * mixed + scores * v) / denominator
        average = jnp.mean(readout, axis=1, keepdims=True)
        centred = readout - average
        variance = jnp.mean(centred * centred, axis=1, keepdims=True)
        normed = centred * lax.rsqrt(variance + head_eps) * gain[block, h : h + 1, :]
        gate = jax.nn.sigmoid(total(3 * cols + at, LANES) * inv)
        hidden[:, at : at + LANES] = (normed * gate).astype(BF16)


def cell(block, own, parts, bias, gain, norm, maxval, matrix, ones, heads_all, features, earlier, last, after):
    rows = own.shape[0]
    real, heads = matrix.shape[:2]
    whole = pl.BlockSpec(memory_space=pltpu.VMEM)
    gates = jax.ShapeDtypeStruct((heads, rows, LANES), F32)
    blocks = block + 1 if last else 1
    earlier = list(earlier) if last else []
    return pl.pallas_call(
        functools.partial(cell_kernel, block, features, heads_all, len(parts), len(earlier) // 2),
        in_specs=[whole] * (7 + len(parts) + len(earlier)) + [pl.BlockSpec(memory_space=pl.ANY)] * len(after),
        out_specs=[whole] * 6,
        out_shape=[
            jax.ShapeDtypeStruct((rows, heads * LANES), BF16),
            jax.ShapeDtypeStruct((blocks,) + norm.shape[1:], F32),
            jax.ShapeDtypeStruct((blocks,) + maxval.shape[1:], F32),
            gates,
            gates,
            gates,
        ],
        scratch_shapes=[
            pltpu.VMEM((rows, heads), F32),
            pltpu.VMEM((heads, rows * 8, LANES), F32),
            pltpu.VMEM((8, LANES), F32),
            pltpu.VMEM((LANES, 8), F32),
        ],
        compiler_params=pltpu.CompilerParams(vmem_limit_bytes=12 << 20),
        cost_estimate=pl.CostEstimate(
            flops=4 * real * heads * LANES * LANES, bytes_accessed=1 << 20, transcendentals=0
        ),
        name="cell",
    )(own, *parts, bias, gain, norm, maxval, in_vmem(matrix), in_vmem(ones), *earlier, *after)


def update_kernel(block, kw, v, dec, matrix, ones, *rest):
    out, buffer, sems = rest[-3:]
    real, heads = matrix.shape[:2]
    pairs = kw.shape[1] // PAD
    moves = spread(pairs, real // pairs)
    copies = []
    for h in range(heads):
        k_high, k_low = pieces(kw[h])
        k_t = columns(k_high, k_high, k_low)
        v_high, v_low = pieces(v[h])
        v_rows = jnp.concatenate([v_high, v_low, v_high, jnp.zeros_like(v_high)], axis=0).astype(BF16)
        for row, seq, count in twos(moves):
            right = jnp.concatenate(
                [ones[:, (row + i) * LANES : (row + i + 1) * LANES] * v_rows for i in range(count)], axis=1
            )
            outer = jnp.dot(k_t, right, preferred_element_type=F32)
            for i in range(count):
                decay = dec[h, row + i : row + i + 1, :]
                buffer[h, seq + i] = decay * matrix[seq + i, h] + outer[:, i * LANES : (i + 1) * LANES]
        copies.append(pltpu.make_async_copy(buffer.at[h], out.at[block, :, h], sems.at[h]))
        copies[-1].start()
    for copy in copies:
        copy.wait()


def update(block, blocks, kw, v, dec, matrix, ones, filled):
    real, heads = matrix.shape[:2]
    whole = pl.BlockSpec(memory_space=pltpu.VMEM)
    aliased = [] if filled is None else [filled]
    return pl.pallas_call(
        functools.partial(update_kernel, block),
        in_specs=[whole] * 5 + [pl.BlockSpec(memory_space=pltpu.HBM)] * len(aliased),
        out_specs=pl.BlockSpec(memory_space=pltpu.HBM),
        out_shape=pltpu.HBM((blocks,) + matrix.shape, F32),
        input_output_aliases={5: 0} if aliased else {},
        scratch_shapes=[
            pltpu.VMEM((heads, real, LANES, LANES), F32),
            pltpu.SemaphoreType.DMA((heads,)),
        ],
        compiler_params=pltpu.CompilerParams(vmem_limit_bytes=12 << 20),
        cost_estimate=pl.CostEstimate(
            flops=8 * real * heads * LANES * LANES,
            bytes_accessed=4 * real * heads * LANES * LANES,
            transcendentals=0,
        ),
        name="update",
    )(kw, v, dec, in_vmem(matrix), in_vmem(ones), *map(in_hbm, aliased))


def output_kernel(slots, meta, w, *refs):
    parts, out = refs[:slots], refs[-1]
    rows = parts[0].shape[0]
    me = meta[0]
    value = jnp.dot(
        jnp.concatenate([part[...] for part in parts], axis=0), w[0], preferred_element_type=F32
    )
    value = value * OUT_UP
    for slot in range(len(parts)):
        start = pl.multiple_of((me ^ slot) * rows, rows)
        out[pl.ds(start, rows), :] = value[slot * rows : (slot + 1) * rows]


def output(block, meta, w, parts, after):
    rows = parts[0].shape[0]
    whole = pl.BlockSpec(memory_space=pltpu.VMEM)
    return pl.pallas_call(
        functools.partial(output_kernel, len(parts)),
        in_specs=[
            pl.BlockSpec(memory_space=pltpu.SMEM),
            pl.BlockSpec((1,) + w.shape[1:], lambda i: (block, 0, 0)),
        ]
        + [whole] * len(parts)
        + [pl.BlockSpec(memory_space=pl.ANY)] * len(after),
        grid=(1,),
        out_specs=whole,
        out_shape=jax.ShapeDtypeStruct((rows * len(parts), w.shape[2]), F32),
        compiler_params=pltpu.CompilerParams(vmem_limit_bytes=12 << 20),
        cost_estimate=pl.CostEstimate(
            flops=2 * rows * len(parts) * w.shape[1] * w.shape[2], bytes_accessed=1 << 20, transcendentals=0
        ),
        name="output",
    )(meta, w, *parts, *after)


def swap(x, axis, size, bit):
    return lax.ppermute(x, axis, [(i, i ^ bit) for i in range(size)])


def on_device(
    tokens,
    w_query,
    w_key,
    w_value,
    w_outgate,
    w_ingate,
    w_forget,
    forget_bias,
    head_gain,
    w_proj,
    mem_matrix,
    mem_norm,
    mem_max,
):
    tp, dp = lax.axis_size("tp"), lax.axis_size("dp")
    real = tokens.shape[0]
    features = tokens.shape[1]
    heads = forget_bias.shape[1]
    heads_all = w_ingate.shape[2]
    assert dp & (dp - 1) == 0 and tp % dp == 0 and real <= PAD and 2 * heads_all <= LANES // 2
    assert tp // dp * PAD == ROWS and heads < heads_all - 2
    meta = jnp.stack([lax.axis_index("dp"), lax.axis_index("tp") * heads]).astype(jnp.int32)

    w_ingate, w_forget = w_ingate.swapaxes(1, 2), w_forget.swapaxes(1, 2)
    mem_max = mem_max.swapaxes(1, 2)
    blocks = w_query.shape[0]
    weights = (w_query, w_key, w_value, w_outgate, w_ingate, w_forget)
    tokens, meta = lax.optimization_barrier((tokens, meta))
    copied, *first = begin(tokens, weights, tp)
    current = lax.all_to_all(copied, "tp", 0, 0)
    earlier, matrix_out, after = [], None, ()
    for block in range(blocks):
        own, *sends = project(block, meta, current, weights if block else first, dp)
        parts = [
            swap(part.astype(jnp.float16), "dp", dp, slot).astype(F32) for slot, part in enumerate(sends, 1)
        ]
        if block == 0:
            state = mem_matrix.shape[1:]
            *matrices, ones = fetch(
                (mem_matrix,), [(0, i, i, None) for i in range(blocks)], [(state, F32)] * blocks, True, (own,)
            )
            after = tuple(matrices)
        hidden, norm_out, max_out, kw, v, dec = cell(
            block, own, parts, forget_bias, head_gain, mem_norm, mem_max, matrices[block], ones,
            heads_all, features * dp, earlier, block + 1 == blocks, after,
        )
        earlier += [norm_out, max_out]
        gathered = [hidden] + [swap(hidden, "dp", dp, slot) for slot in range(1, dp)]
        matrix_out = update(block, blocks, kw, v, dec, matrices[block], ones, matrix_out)
        after = (in_hbm(matrix_out),)
        partial = output(block, meta, w_proj, gathered, after if block + 1 == blocks else ()).reshape(tp, PAD, features)
        summed = lax.all_to_all(partial.astype(jnp.float16), "tp", 0, 0)
        summed = (jnp.sum(summed.astype(F32), axis=0) * (1.0 / OUT_UP)).astype(BF16)
        if block + 1 < blocks:
            current = lax.all_to_all(jnp.broadcast_to(summed[None], (tp,) + summed.shape), "tp", 0, 0)
    return (summed[:real], matrix_out, norm_out, max_out.swapaxes(1, 2))


def solution(mesh):
    in_specs = (
        P("tp", "dp"),
        P(None, "dp", "tp"),
        P(None, "dp", "tp"),
        P(None, "dp", "tp"),
        P(None, "dp", "tp"),
        P(None, "dp", None),
        P(None, "dp", None),
        P(None, "tp"),
        P(None, "tp", None),
        P(None, "tp", "dp"),
        P(None, "dp", "tp", None, None),
        P(None, "dp", "tp", None),
        P(None, "dp", "tp"),
    )
    out_specs = (
        P("tp", "dp"),
        P(None, "dp", "tp", None, None),
        P(None, "dp", "tp", None),
        P(None, "dp", "tp"),
    )
    return jax.shard_map(
        on_device, mesh=mesh, in_specs=in_specs, out_specs=out_specs, check_vma=False
    )
```

```python
import functools

import jax
import jax.numpy as jnp
from jax import lax
from jax.experimental import pallas as pl
from jax.experimental.pallas import tpu as pltpu
from jax.sharding import PartitionSpec as P

norm_eps = 1e-06
head_eps = 1e-05
ROWS = 32
PAD = 16
LANES = 128
UP = 12.0
TINY = 1e-30
OUT_UP = 16.0
F32 = jnp.float32
BF16 = jnp.bfloat16


def in_hbm(x):
    return pltpu.with_memory_space_constraint(x, pltpu.HBM)


def in_vmem(x):
    return pltpu.with_memory_space_constraint(x, pltpu.VMEM)


def lane_roll(x, amount):
    return pltpu.roll(x, amount % x.shape[-1], 1)


def fetch_kernel(steps, count, *refs):
    sources, targets, sems = refs[:count], refs[-1 - steps[1] : -1], refs[-1]
    copies = []
    for source, part, target, place in steps[0]:
        from_ref = sources[source] if part is None else sources[source].at[part]
        to_ref = targets[target] if place is None else targets[target].at[place]
        copies.append(pltpu.make_async_copy(from_ref, to_ref, sems.at[len(copies)]))
    for copy in copies:
        copy.start()
    if steps[2]:
        ones = targets[-1]
        for block in range(ones.shape[1] // LANES):
            row = lax.broadcasted_iota(jnp.int32, (LANES, LANES), 0)
            here = (row % ROWS == block) & (row < 3 * ROWS)
            ones[:, block * LANES : (block + 1) * LANES] = jnp.where(here, 1.0, 0.0).astype(BF16)
    for copy in copies:
        copy.wait()


def fetch(arrays, steps, shapes, with_ones=False, after=()):
    shapes = list(shapes)
    if with_ones:
        shapes.append(((LANES, ROWS * LANES), BF16))
    total = sum(a.size * a.dtype.itemsize for a in arrays)
    return pl.pallas_call(
        functools.partial(fetch_kernel, (steps, len(shapes), with_ones), len(arrays)),
        in_specs=[pl.BlockSpec(memory_space=pltpu.HBM)] * len(arrays)
        + [pl.BlockSpec(memory_space=pl.ANY)] * len(after),
        out_specs=[pl.BlockSpec(memory_space=pltpu.VMEM)] * len(shapes),
        out_shape=[pltpu.VMEM(shape, dtype) for shape, dtype in shapes],
        scratch_shapes=[pltpu.SemaphoreType.DMA((len(steps),))],
        compiler_params=pltpu.CompilerParams(vmem_limit_bytes=8 << 20),
        cost_estimate=pl.CostEstimate(flops=total, bytes_accessed=total, transcendentals=0),
        name="fetch",
    )(*map(in_hbm, arrays), *after)


def begin_kernel(tokens, *refs):
    count = (len(refs) - 2) // 2
    sources, (copied, *targets), sems = refs[:count], refs[count:-1], refs[-1]
    moves = [(tokens, copied.at[i]) for i in range(copied.shape[0])]
    moves += [(source.at[:1], target) for source, target in zip(sources, targets)]
    copies = [
        pltpu.make_async_copy(source, target, sems.at[i]) for i, (source, target) in enumerate(moves)
    ]
    for copy in copies:
        copy.start()
    for copy in copies:
        copy.wait()


def begin(tokens, weights, copies):
    shapes = [((copies,) + tokens.shape, BF16)] + [((1,) + w.shape[1:], BF16) for w in weights]
    whole = pl.BlockSpec(memory_space=pltpu.VMEM)
    return pl.pallas_call(
        begin_kernel,
        in_specs=[pl.BlockSpec(memory_space=pltpu.HBM)] * (1 + len(weights)),
        out_specs=[whole] * len(shapes),
        out_shape=[pltpu.VMEM(shape, dtype) for shape, dtype in shapes],
        scratch_shapes=[pltpu.SemaphoreType.DMA((copies + len(weights),))],
        compiler_params=pltpu.CompilerParams(vmem_limit_bytes=8 << 20),
        name="begin",
    )(*map(in_hbm, (tokens,) + weights))


def first_project_kernel(block, heads_all, meta, x, wq, wk, wi, wf, keep, send, x_rel, gates):
    rows = ROWS
    slots = x_rel.shape[0] // rows
    me = meta[0]
    first_head = meta[1]
    pairs, real = rows // PAD, x.shape[1]
    if real < PAD:
        x_rel[...] = jnp.zeros(x_rel.shape, BF16)
    for place, slot in enumerate(slot_order(slots)):
        for i in range(pairs):
            at = place * rows + i * PAD
            x_rel[at : at + real, :] = x[(me ^ slot) * pairs + i]
    xs = x_rel[...]
    cols = wq.shape[2]
    half = keep.shape[0]

    def emit(value, offset):
        width = value.shape[1]
        keep[:, offset : offset + width] = value[:half]
        send[:, offset : offset + width] = value[half:]

    for index, weight in enumerate((wq, wk)):
        emit(jnp.dot(xs, weight[block], preferred_element_type=F32), index * cols)
    wide = xs.astype(F32)
    squares = jnp.sum(wide * wide, axis=1, keepdims=True)
    gates[...] = jnp.zeros(gates.shape, F32)
    for index, weight in enumerate((wi, wf)):
        value = lax.dot_general(xs, weight[block], (((1,), (1,)), ((), ())), preferred_element_type=F32)
        gates[:, index * heads_all : (index + 1) * heads_all] = value
    lane = lax.broadcasted_iota(jnp.int32, gates.shape, 1)
    mine = pltpu.roll(gates[...], (LANES - first_head) % LANES, 1)
    emit(jnp.where(lane == heads_all - 1, squares, mine), 2 * cols)


def second_project_kernel(block, x_rel, wv, wo, keep, send):
    xs = x_rel[...]
    cols = wv.shape[2]
    half = keep.shape[0]
    for index, weight in enumerate((wv, wo)):
        value = jnp.dot(xs, weight[block], preferred_element_type=F32)
        keep[:, index * cols : (index + 1) * cols] = value[:half]
        send[:, index * cols : (index + 1) * cols] = value[half:]


def first_add_kernel(heads_all, keep, other, scale_out, *outs):
    wide = keep.shape[1]
    tile = keep[:, wide - LANES :] + other[:, wide - LANES :]
    squares = tile[:, heads_all - 1 : heads_all]
    power = jnp.floor(0.5 * jnp.log2(squares + TINY))
    scale = jnp.exp2(UP - power)
    scale_out[...] = jnp.broadcast_to(scale, scale_out.shape)
    lane = lax.broadcasted_iota(jnp.int32, tile.shape, 1)
    tile = tile * scale
    tile = jnp.where(lane == heads_all - 1, squares * jnp.exp2(-2.0 * power), tile)
    tile = jnp.where(lane == heads_all - 2, power, tile)
    low = tile - tile.astype(BF16).astype(F32)
    tile = jnp.where(lane < LANES // 2, tile, pltpu.roll(low, LANES // 2, 1))
    for i, out in enumerate(outs):
        at = slice(i * ROWS, (i + 1) * ROWS)
        out[:, : wide - LANES] = (keep[at, : wide - LANES] + other[at, : wide - LANES]) * scale[at]
        out[:, wide - LANES :] = tile[at]


def second_add_kernel(keep, other, scale, *outs):
    for i, out in enumerate(outs):
        at = slice(i * ROWS, (i + 1) * ROWS)
        out[...] = (keep[at] + other[at]) * scale[at, :1]


def slot_order(slots):
    return list(range(0, slots, 2)) + list(range(1, slots, 2))


def small_call(kernel, name, shapes, args, scratch=(), scalars=0, flops=0):
    whole = pl.BlockSpec(memory_space=pltpu.VMEM)
    return pl.pallas_call(
        kernel,
        in_specs=[pl.BlockSpec(memory_space=pltpu.SMEM)] * scalars + [whole] * (len(args) - scalars),
        out_specs=[whole] * len(shapes),
        out_shape=[jax.ShapeDtypeStruct(shape, dtype) for shape, dtype in shapes],
        scratch_shapes=list(scratch),
        compiler_params=pltpu.CompilerParams(vmem_limit_bytes=8 << 20),
        cost_estimate=pl.CostEstimate(flops=flops, bytes_accessed=1 << 20, transcendentals=0),
        name=name,
    )(*args)


def project(block, meta, x, weights, slots):
    wq, wk, wv, wo, wi, wf = map(in_vmem, weights)
    all_rows, features = slots * ROWS, x.shape[2]
    half = all_rows // 2
    cols, heads_all = wq.shape[2], wi.shape[1]
    first, second = 2 * cols + LANES, 2 * cols
    flops = 2 * all_rows * features * second
    keep_a, send_a, x_rel = small_call(
        functools.partial(first_project_kernel, block, heads_all),
        "project_first",
        [((half, first), F32)] * 2 + [((all_rows, features), BF16)],
        (meta, x, wq, wk, wi, wf),
        [pltpu.VMEM((all_rows, LANES), F32)],
        1,
        flops,
    )
    other_a = swap(send_a, "dp", slots, 1)
    keep_b, send_b = small_call(
        functools.partial(second_project_kernel, block),
        "project_second",
        [((half, second), F32)] * 2,
        (x_rel, wv, wo),
        flops=flops,
    )
    other_b = swap(send_b, "dp", slots, 1)
    scale, *sums_a = small_call(
        functools.partial(first_add_kernel, heads_all),
        "add_first",
        [((half, LANES), F32)] + [((ROWS, first), F32)] * (slots // 2),
        (keep_a, other_a),
        flops=1 << 20,
    )
    sums_b = small_call(
        second_add_kernel, "add_second", [((ROWS, second), F32)] * (slots // 2), (keep_b, other_b, scale), flops=1 << 20
    )

    def across(sums):
        return [sums[0]] + [
            swap(part.astype(jnp.float16), "dp", slots, slot).astype(F32)
            for part, slot in zip(sums[1:], range(2, slots, 2))
        ]

    return across(sums_a), across(sums_b)


def spread(pairs, real):
    return [(slice(i * PAD, i * PAD + real), slice(i * real, (i + 1) * real)) for i in range(pairs)]


def twos(moves):
    runs = []
    for padded, plain in moves:
        length = plain.stop - plain.start
        for j in range(0, length, 2):
            runs.append((padded.start + j, plain.start + j, min(2, length - j)))
    return runs


def pieces(x):
    high = x.astype(BF16).astype(F32)
    return high, x - high


def columns(*parts):
    parts = list(parts)
    rest = LANES - sum(part.shape[0] for part in parts)
    if rest:
        parts.append(jnp.zeros((rest, LANES), F32))
    return jnp.concatenate(parts, axis=0).T.astype(BF16)


def cell_kernel(block, features, heads_all, peers, before, *refs):
    firsts, seconds = refs[:peers], refs[peers : 2 * peers]
    bias, gain, norm, maxval, matrix, ones = refs[2 * peers : 2 * peers + 6]
    earlier = refs[2 * peers + 6 : 2 * peers + 6 + 2 * before]
    (hidden, norm_out, max_out, kw_out, v_out, dec_out, mp_s, part_s, wide_s, tall_s) = refs[-10:]
    heads = matrix.shape[1]
    rows, real = hidden.shape[0], matrix.shape[0]
    pairs = rows // PAD
    moves = spread(pairs, real // pairs)
    cols = heads * LANES

    for i in range(before):
        norm_out[i] = earlier[2 * i][0]
        max_out[i] = earlier[2 * i + 1][0]
    norm_out, max_out = norm_out.at[before], max_out.at[before]

    scales, packed, squares = [], 0.0, 0.0
    for part in firsts:
        tile = part[:, 2 * cols :]
        tile = tile + lane_roll(tile, LANES // 2)
        power = tile[:, heads_all - 2 : heads_all - 1]
        scales.append(jnp.exp2(power - UP))
        packed = packed + tile * scales[-1]
        squares = squares + tile[:, heads_all - 1 : heads_all] * jnp.exp2(2.0 * power)

    def total(parts, start):
        value = 0.0
        for part, scale in zip(parts, scales):
            value = value + part[:, start : start + LANES] * scale
        return value

    inv = lax.rsqrt(squares / features + norm_eps)
    log_in = packed[:, :heads] * inv
    raw = packed[:, heads_all : heads_all + heads] * inv + bias[block : block + 1, :]
    log_forget = jnp.minimum(raw, 0.0) - jnp.log1p(jnp.exp(-jnp.abs(raw)))
    mp_s[...] = jnp.zeros(mp_s.shape, F32)
    tall_s[...] = jnp.zeros(tall_s.shape, F32)
    wide_s[...] = jnp.zeros(wide_s.shape, F32)
    wide_s[:heads, :real] = maxval[block]
    tall = wide_s[...].T
    for padded, plain in moves:
        mp_s[padded, :] = tall[plain, :heads]
    carried = log_forget + mp_s[...]
    new_max = jnp.maximum(carried, log_in)
    decays = jnp.exp(carried - new_max)
    weight_in = jnp.exp(log_in - new_max)
    for padded, plain in moves:
        tall_s[plain, :heads] = new_max[padded]
    max_out[...] = tall_s[...].T[:heads, :real]
    part_s[...] = jnp.zeros(part_s.shape, F32)
    for h in range(heads):
        at = h * LANES
        q = total(firsts, at) * inv
        high, rest = pieces(q)
        middle, low = pieces(rest)
        q_t = columns(high, middle, low)
        for row, seq, count in twos(moves):
            spread_q = jnp.dot(
                q_t, ones[:, row * LANES : (row + count) * LANES], preferred_element_type=F32
            )
            for i in range(count):
                product = matrix[seq + i, h] * spread_q[:, i * LANES : (i + 1) * LANES]
                part_s[h, (row + i) * 8 : (row + i) * 8 + 8, :] = jnp.sum(
                    product.reshape(LANES // 8, 8, LANES), axis=0
                )
        v = total(seconds, at) * inv
        v_out[h] = v
        dec = jnp.broadcast_to(decays[:, h : h + 1], (rows, LANES))
        dec_out[h] = dec
        kw = total(firsts, cols + at) * (inv * LANES ** (-0.5)) * weight_in[:, h : h + 1]
        kw_out[h] = kw
        for padded, plain in moves:
            nn = dec[padded] * norm[block, plain, h, :] + kw[padded]
            norm_out[plain, h, :] = nn
            mp_s[padded, h : h + 1] = jnp.sum(q[padded] * nn, axis=1, keepdims=True)
        denominator = jnp.maximum(jnp.abs(mp_s[:, h : h + 1]), 1.0)
        mixed = part_s[h, pl.ds(0, rows, stride=8), :]
        for j in range(1, 8):
            mixed = mixed + part_s[h, pl.ds(j, rows, stride=8), :]
        scores = jnp.sum(q * kw, axis=1, keepdims=True)
        readout = (dec * mixed + scores * v) / denominator
        average = jnp.mean(readout, axis=1, keepdims=True)
        centred = readout - average
        variance = jnp.mean(centred * centred, axis=1, keepdims=True)
        normed = centred * lax.rsqrt(variance + head_eps) * gain[block, h : h + 1, :]
        gate = jax.nn.sigmoid(total(seconds, cols + at) * inv)
        hidden[:, at : at + LANES] = (normed * gate).astype(BF16)


def cell(block, firsts, seconds, bias, gain, norm, maxval, matrix, ones, heads_all, features, earlier, last, after):
    rows = firsts[0].shape[0]
    real, heads = matrix.shape[:2]
    whole = pl.BlockSpec(memory_space=pltpu.VMEM)
    gates = jax.ShapeDtypeStruct((heads, rows, LANES), F32)
    blocks = block + 1 if last else 1
    earlier = list(earlier) if last else []
    return pl.pallas_call(
        functools.partial(cell_kernel, block, features, heads_all, len(firsts), len(earlier) // 2),
        in_specs=[whole] * (6 + 2 * len(firsts) + len(earlier)) + [pl.BlockSpec(memory_space=pl.ANY)] * len(after),
        out_specs=[whole] * 6,
        out_shape=[
            jax.ShapeDtypeStruct((rows, heads * LANES), BF16),
            jax.ShapeDtypeStruct((blocks,) + norm.shape[1:], F32),
            jax.ShapeDtypeStruct((blocks,) + maxval.shape[1:], F32),
            gates,
            gates,
            gates,
        ],
        scratch_shapes=[
            pltpu.VMEM((rows, heads), F32),
            pltpu.VMEM((heads, rows * 8, LANES), F32),
            pltpu.VMEM((8, LANES), F32),
            pltpu.VMEM((LANES, 8), F32),
        ],
        compiler_params=pltpu.CompilerParams(vmem_limit_bytes=12 << 20),
        cost_estimate=pl.CostEstimate(
            flops=4 * real * heads * LANES * LANES, bytes_accessed=1 << 20, transcendentals=0
        ),
        name="cell",
    )(*firsts, *seconds, bias, gain, norm, maxval, in_vmem(matrix), in_vmem(ones), *earlier, *after)


def update_kernel(block, kw, v, dec, matrix, ones, *rest):
    out, buffer, sems = rest[-3:]
    real, heads = matrix.shape[:2]
    pairs = kw.shape[1] // PAD
    moves = spread(pairs, real // pairs)
    copies = []
    for h in range(heads):
        k_high, k_low = pieces(kw[h])
        k_t = columns(k_high, k_high, k_low)
        v_high, v_low = pieces(v[h])
        v_rows = jnp.concatenate([v_high, v_low, v_high, jnp.zeros_like(v_high)], axis=0).astype(BF16)
        for row, seq, count in twos(moves):
            right = jnp.concatenate(
                [ones[:, (row + i) * LANES : (row + i + 1) * LANES] * v_rows for i in range(count)], axis=1
            )
            outer = jnp.dot(k_t, right, preferred_element_type=F32)
            for i in range(count):
                decay = dec[h, row + i : row + i + 1, :]
                buffer[h, seq + i] = decay * matrix[seq + i, h] + outer[:, i * LANES : (i + 1) * LANES]
        copies.append(pltpu.make_async_copy(buffer.at[h], out.at[block, :, h], sems.at[h]))
        copies[-1].start()
    for copy in copies:
        copy.wait()


def update(block, blocks, kw, v, dec, matrix, ones, filled):
    real, heads = matrix.shape[:2]
    whole = pl.BlockSpec(memory_space=pltpu.VMEM)
    aliased = [] if filled is None else [filled]
    return pl.pallas_call(
        functools.partial(update_kernel, block),
        in_specs=[whole] * 5 + [pl.BlockSpec(memory_space=pltpu.HBM)] * len(aliased),
        out_specs=pl.BlockSpec(memory_space=pltpu.HBM),
        out_shape=pltpu.HBM((blocks,) + matrix.shape, F32),
        input_output_aliases={5: 0} if aliased else {},
        scratch_shapes=[
            pltpu.VMEM((heads, real, LANES, LANES), F32),
            pltpu.SemaphoreType.DMA((heads,)),
        ],
        compiler_params=pltpu.CompilerParams(vmem_limit_bytes=12 << 20),
        cost_estimate=pl.CostEstimate(
            flops=8 * real * heads * LANES * LANES,
            bytes_accessed=4 * real * heads * LANES * LANES,
            transcendentals=0,
        ),
        name="update",
    )(kw, v, dec, in_vmem(matrix), in_vmem(ones), *map(in_hbm, aliased))


def output_kernel(slots, meta, w, *refs):
    parts, out = refs[:slots], refs[-1]
    rows = parts[0].shape[0]
    me = meta[0]
    value = jnp.dot(
        jnp.concatenate([part[...] for part in parts], axis=0), w[0], preferred_element_type=F32
    )
    value = value * OUT_UP
    for slot in range(len(parts)):
        start = pl.multiple_of((me ^ slot) * rows, rows)
        out[pl.ds(start, rows), :] = value[slot * rows : (slot + 1) * rows]


def output(block, meta, w, parts, after):
    rows = parts[0].shape[0]
    whole = pl.BlockSpec(memory_space=pltpu.VMEM)
    return pl.pallas_call(
        functools.partial(output_kernel, len(parts)),
        in_specs=[
            pl.BlockSpec(memory_space=pltpu.SMEM),
            pl.BlockSpec((1,) + w.shape[1:], lambda i: (block, 0, 0)),
        ]
        + [whole] * len(parts)
        + [pl.BlockSpec(memory_space=pl.ANY)] * len(after),
        grid=(1,),
        out_specs=whole,
        out_shape=jax.ShapeDtypeStruct((rows * len(parts), w.shape[2]), F32),
        compiler_params=pltpu.CompilerParams(vmem_limit_bytes=12 << 20),
        cost_estimate=pl.CostEstimate(
            flops=2 * rows * len(parts) * w.shape[1] * w.shape[2], bytes_accessed=1 << 20, transcendentals=0
        ),
        name="output",
    )(meta, w, *parts, *after)


def swap(x, axis, size, bit):
    return lax.ppermute(x, axis, [(i, i ^ bit) for i in range(size)])


def on_device(
    tokens,
    w_query,
    w_key,
    w_value,
    w_outgate,
    w_ingate,
    w_forget,
    forget_bias,
    head_gain,
    w_proj,
    mem_matrix,
    mem_norm,
    mem_max,
):
    tp, dp = lax.axis_size("tp"), lax.axis_size("dp")
    real = tokens.shape[0]
    features = tokens.shape[1]
    heads = forget_bias.shape[1]
    heads_all = w_ingate.shape[2]
    assert dp & (dp - 1) == 0 and tp % dp == 0 and real <= PAD and 2 * heads_all <= LANES // 2
    assert tp // dp * PAD == ROWS and heads < heads_all - 2
    meta = jnp.stack([lax.axis_index("dp"), lax.axis_index("tp") * heads]).astype(jnp.int32)

    w_ingate, w_forget = w_ingate.swapaxes(1, 2), w_forget.swapaxes(1, 2)
    mem_max = mem_max.swapaxes(1, 2)
    blocks = w_query.shape[0]
    weights = (w_query, w_key, w_value, w_outgate, w_ingate, w_forget)
    tokens, meta = lax.optimization_barrier((tokens, meta))
    copied, *first = begin(tokens, weights, tp)
    current = lax.all_to_all(copied, "tp", 0, 0)
    earlier, matrix_out, after = [], None, ()
    for block in range(blocks):
        firsts, seconds = project(block, meta, current, weights if block else first, dp)
        state = [(mem_matrix.shape[1:], F32)]
        if block == 0:
            *matrices, ones = fetch((mem_matrix,), [(0, 0, 0, None)], state, True, (seconds[0],))
            after = tuple(matrices)
        hidden, norm_out, max_out, kw, v, dec = cell(
            block, firsts, seconds, forget_bias, head_gain, mem_norm, mem_max, matrices[block], ones,
            heads_all, features * dp, earlier, block + 1 == blocks, after,
        )
        earlier += [norm_out, max_out]
        gathered = [hidden] + [swap(hidden, "dp", dp, slot) for slot in range(1, dp)]
        matrix_out = update(block, blocks, kw, v, dec, matrices[block], ones, matrix_out)
        after = (in_hbm(matrix_out),)
        fillers = after
        if block + 1 < blocks:
            fillers = fetch((mem_matrix,), [(0, block + 1, 0, None)], state, False, (hidden,))
            matrices += fillers
        partial = output(block, meta, w_proj, gathered, tuple(fillers)).reshape(tp, PAD, features)
        summed = lax.all_to_all(partial.astype(jnp.float16), "tp", 0, 0)
        summed = (jnp.sum(summed.astype(F32), axis=0) * (1.0 / OUT_UP)).astype(BF16)
        if block + 1 < blocks:
            current = lax.all_to_all(jnp.broadcast_to(summed[None], (tp,) + summed.shape), "tp", 0, 0)
    return (summed[:real], matrix_out, norm_out, max_out.swapaxes(1, 2))


def solution(mesh):
    in_specs = (
        P("tp", "dp"),
        P(None, "dp", "tp"),
        P(None, "dp", "tp"),
        P(None, "dp", "tp"),
        P(None, "dp", "tp"),
        P(None, "dp", None),
        P(None, "dp", None),
        P(None, "tp"),
        P(None, "tp", None),
        P(None, "tp", "dp"),
        P(None, "dp", "tp", None, None),
        P(None, "dp", "tp", None),
        P(None, "dp", "tp"),
    )
    out_specs = (
        P("tp", "dp"),
        P(None, "dp", "tp", None, None),
        P(None, "dp", "tp", None),
        P(None, "dp", "tp"),
    )
    return jax.shard_map(
        on_device, mesh=mesh, in_specs=in_specs, out_specs=out_specs, check_vma=False
    )
```

```python
import functools

import jax
import jax.numpy as jnp
from jax import lax
from jax.experimental import pallas as pl
from jax.experimental.pallas import tpu as pltpu
from jax.sharding import PartitionSpec as P

norm_eps = 1e-06
head_eps = 1e-05
ROWS = 32
PAD = 16
LANES = 128
UP = 12.0
TINY = 1e-30
STORES = 2
OUT_UP = 16.0
F32 = jnp.float32
BF16 = jnp.bfloat16


def in_hbm(x):
    return pltpu.with_memory_space_constraint(x, pltpu.HBM)


def in_vmem(x):
    return pltpu.with_memory_space_constraint(x, pltpu.VMEM)


def lane_roll(x, amount):
    return pltpu.roll(x, amount % x.shape[-1], 1)


def fetch_kernel(steps, count, *refs):
    sources, targets, sems = refs[:count], refs[-1 - steps[1] : -1], refs[-1]
    copies = []
    for source, part, target, place in steps[0]:
        from_ref = sources[source] if part is None else sources[source].at[part]
        to_ref = targets[target] if place is None else targets[target].at[place]
        copies.append(pltpu.make_async_copy(from_ref, to_ref, sems.at[len(copies)]))
    for copy in copies:
        copy.start()
    if steps[2]:
        ones = targets[-1]
        for block in range(ones.shape[1] // LANES):
            row = lax.broadcasted_iota(jnp.int32, (LANES, LANES), 0)
            here = (row % ROWS == block) & (row < 3 * ROWS)
            ones[:, block * LANES : (block + 1) * LANES] = jnp.where(here, 1.0, 0.0).astype(BF16)
    for copy in copies:
        copy.wait()


def fetch(arrays, steps, shapes, with_ones=False, after=()):
    shapes = list(shapes)
    if with_ones:
        shapes.append(((LANES, ROWS * LANES), BF16))
    total = sum(a.size * a.dtype.itemsize for a in arrays)
    return pl.pallas_call(
        functools.partial(fetch_kernel, (steps, len(shapes), with_ones), len(arrays)),
        in_specs=[pl.BlockSpec(memory_space=pltpu.HBM)] * len(arrays)
        + [pl.BlockSpec(memory_space=pl.ANY)] * len(after),
        out_specs=[pl.BlockSpec(memory_space=pltpu.VMEM)] * len(shapes),
        out_shape=[pltpu.VMEM(shape, dtype) for shape, dtype in shapes],
        scratch_shapes=[pltpu.SemaphoreType.DMA((len(steps),))],
        compiler_params=pltpu.CompilerParams(vmem_limit_bytes=8 << 20),
        cost_estimate=pl.CostEstimate(flops=total, bytes_accessed=total, transcendentals=0),
        name="fetch",
    )(*map(in_hbm, arrays), *after)


def begin_kernel(tokens, *refs):
    count = (len(refs) - 2) // 2
    sources, (copied, *targets), sems = refs[:count], refs[count:-1], refs[-1]
    moves = [(tokens, copied.at[i]) for i in range(copied.shape[0])]
    moves += [(source.at[:1], target) for source, target in zip(sources, targets)]
    copies = [
        pltpu.make_async_copy(source, target, sems.at[i]) for i, (source, target) in enumerate(moves)
    ]
    for copy in copies:
        copy.start()
    for copy in copies:
        copy.wait()


def begin(tokens, weights, copies):
    shapes = [((copies,) + tokens.shape, BF16)] + [((1,) + w.shape[1:], BF16) for w in weights]
    whole = pl.BlockSpec(memory_space=pltpu.VMEM)
    return pl.pallas_call(
        begin_kernel,
        in_specs=[pl.BlockSpec(memory_space=pltpu.HBM)] * (1 + len(weights)),
        out_specs=[whole] * len(shapes),
        out_shape=[pltpu.VMEM(shape, dtype) for shape, dtype in shapes],
        scratch_shapes=[pltpu.SemaphoreType.DMA((copies + len(weights),))],
        compiler_params=pltpu.CompilerParams(vmem_limit_bytes=8 << 20),
        name="begin",
    )(*map(in_hbm, (tokens,) + weights))


def first_project_kernel(block, heads_all, heads, x, wq, wk, wi, wf, *rest):
    later = (len(rest) - 5) // 2
    keep, send, x_rel, gates = rest[later : later + 3] + (rest[2 * later + 3],)
    copies = []
    for source, target in zip(rest[:later], rest[later + 3 : 2 * later + 3]):
        copies.append(pltpu.make_async_copy(source.at[:1], target, rest[-1].at[len(copies)]))
        copies[-1].start()
    rows = ROWS
    slots = x_rel.shape[0] // rows
    me = lax.axis_index("dp")
    first_head = lax.axis_index("tp") * heads
    pairs, real = rows // PAD, x.shape[1]
    if real < PAD:
        x_rel[...] = jnp.zeros(x_rel.shape, BF16)
    for place, slot in enumerate(slot_order(slots)):
        for i in range(pairs):
            at = place * rows + i * PAD
            x_rel[at : at + real, :] = x[(me ^ slot) * pairs + i]
    xs = x_rel[...]
    cols = wq.shape[2]
    half = keep.shape[0]

    def emit(value, offset):
        width = value.shape[1]
        keep[:, offset : offset + width] = value[:half]
        send[:, offset : offset + width] = value[half:]

    for index, weight in enumerate((wq, wk)):
        emit(jnp.dot(xs, weight[block], preferred_element_type=F32), index * cols)
    wide = xs.astype(F32)
    squares = jnp.sum(wide * wide, axis=1, keepdims=True)
    gates[...] = jnp.zeros(gates.shape, F32)
    for index, weight in enumerate((wi, wf)):
        value = lax.dot_general(xs, weight[block], (((1,), (1,)), ((), ())), preferred_element_type=F32)
        gates[:, index * heads_all : (index + 1) * heads_all] = value
    lane = lax.broadcasted_iota(jnp.int32, gates.shape, 1)
    mine = pltpu.roll(gates[...], (LANES - first_head) % LANES, 1)
    emit(jnp.where(lane == heads_all - 1, squares, mine), 2 * cols)
    for copy in copies:
        copy.wait()


def second_project_kernel(block, x_rel, wv, wo, keep, send):
    xs = x_rel[...]
    cols = wv.shape[2]
    half = keep.shape[0]
    for index, weight in enumerate((wv, wo)):
        value = jnp.dot(xs, weight[block], preferred_element_type=F32)
        keep[:, index * cols : (index + 1) * cols] = value[:half]
        send[:, index * cols : (index + 1) * cols] = value[half:]


def first_add_kernel(heads_all, keep, other, scale_out, *outs):
    wide = keep.shape[1]
    tile = keep[:, wide - LANES :] + other[:, wide - LANES :]
    squares = tile[:, heads_all - 1 : heads_all]
    power = jnp.floor(0.5 * jnp.log2(squares + TINY))
    scale = jnp.exp2(UP - power)
    scale_out[...] = jnp.broadcast_to(scale, scale_out.shape)
    lane = lax.broadcasted_iota(jnp.int32, tile.shape, 1)
    tile = tile * scale
    tile = jnp.where(lane == heads_all - 1, squares * jnp.exp2(-2.0 * power), tile)
    tile = jnp.where(lane == heads_all - 2, power, tile)
    low = tile - tile.astype(BF16).astype(F32)
    tile = jnp.where(lane < LANES // 2, tile, pltpu.roll(low, LANES // 2, 1))
    for i, out in enumerate(outs):
        at = slice(i * ROWS, (i + 1) * ROWS)
        out[:, : wide - LANES] = (keep[at, : wide - LANES] + other[at, : wide - LANES]) * scale[at]
        out[:, wide - LANES :] = tile[at]


def second_add_kernel(keep, other, scale, *outs):
    for i, out in enumerate(outs):
        at = slice(i * ROWS, (i + 1) * ROWS)
        out[...] = (keep[at] + other[at]) * scale[at, :1]


def slot_order(slots):
    return list(range(0, slots, 2)) + list(range(1, slots, 2))


def small_call(kernel, name, shapes, args, scratch=(), in_place=0, flops=0):
    whole = pl.BlockSpec(memory_space=pltpu.VMEM)
    return pl.pallas_call(
        kernel,
        in_specs=[whole] * (len(args) - in_place) + [pl.BlockSpec(memory_space=pltpu.HBM)] * in_place,
        out_specs=[whole] * len(shapes),
        out_shape=[pltpu.VMEM(shape, dtype) for shape, dtype in shapes],
        scratch_shapes=list(scratch),
        compiler_params=pltpu.CompilerParams(vmem_limit_bytes=8 << 20),
        cost_estimate=pl.CostEstimate(flops=flops, bytes_accessed=1 << 20, transcendentals=0),
        name=name,
    )(*args)


def project(block, heads, x, weights, later, slots):
    wq, wk, wi, wf, *others = map(in_vmem, weights)
    later = [in_hbm(w) for w in later]
    all_rows, features = slots * ROWS, x.shape[2]
    half = all_rows // 2
    cols, heads_all = wq.shape[2], wi.shape[1]
    first, second = 2 * cols + LANES, 2 * cols
    flops = 2 * all_rows * features * second
    scratch = [pltpu.VMEM((all_rows, LANES), F32), pltpu.SemaphoreType.DMA((max(len(later), 1),))]
    keep_a, send_a, x_rel, *fetched = small_call(
        functools.partial(first_project_kernel, block, heads_all, heads),
        "project_first",
        [((half, first), F32)] * 2
        + [((all_rows, features), BF16)]
        + [((1,) + w.shape[1:], BF16) for w in later],
        (x, wq, wk, wi, wf, *later),
        scratch,
        len(later),
        flops,
    )
    wv, wo = fetched or others
    other_a = swap(send_a, "dp", slots, 1)
    keep_b, send_b = small_call(
        functools.partial(second_project_kernel, block),
        "project_second",
        [((half, second), F32)] * 2,
        (x_rel, wv, wo),
        flops=flops,
    )
    other_b = swap(send_b, "dp", slots, 1)
    scale, *sums_a = small_call(
        functools.partial(first_add_kernel, heads_all),
        "add_first",
        [((half, LANES), F32)] + [((ROWS, first), F32)] * (slots // 2),
        (keep_a, other_a),
        flops=1 << 20,
    )
    sums_b = small_call(
        second_add_kernel, "add_second", [((ROWS, second), F32)] * (slots // 2), (keep_b, other_b, scale), flops=1 << 20
    )

    def across(sums):
        return [sums[0]] + [
            swap(part.astype(jnp.float16), "dp", slots, slot).astype(F32)
            for part, slot in zip(sums[1:], range(2, slots, 2))
        ]

    return across(sums_a), across(sums_b)


def spread(pairs, real):
    return [(slice(i * PAD, i * PAD + real), slice(i * real, (i + 1) * real)) for i in range(pairs)]


def twos(moves):
    runs = []
    for padded, plain in moves:
        length = plain.stop - plain.start
        for j in range(0, length, 2):
            runs.append((padded.start + j, plain.start + j, min(2, length - j)))
    return runs


def pieces(x):
    high = x.astype(BF16).astype(F32)
    return high, x - high


def columns(*parts):
    parts = list(parts)
    rest = LANES - sum(part.shape[0] for part in parts)
    if rest:
        parts.append(jnp.zeros((rest, LANES), F32))
    return jnp.concatenate(parts, axis=0).T.astype(BF16)


def cell_kernel(block, features, heads_all, peers, before, *refs):
    firsts, seconds = refs[:peers], refs[peers : 2 * peers]
    bias, gain, norm, maxval, matrix, ones = refs[2 * peers : 2 * peers + 6]
    earlier = refs[2 * peers + 6 : 2 * peers + 6 + 2 * before]
    (hidden, norm_out, max_out, kw_out, v_out, dec_out, mp_s, part_s, wide_s, tall_s) = refs[-10:]
    heads = matrix.shape[1]
    rows, real = hidden.shape[0], matrix.shape[0]
    pairs = rows // PAD
    moves = spread(pairs, real // pairs)
    cols = heads * LANES

    for i in range(before):
        norm_out[i] = earlier[2 * i][0]
        max_out[i] = earlier[2 * i + 1][0]
    norm_out, max_out = norm_out.at[before], max_out.at[before]

    scales, packed, squares = [], 0.0, 0.0
    for part in firsts:
        tile = part[:, 2 * cols :]
        tile = tile + lane_roll(tile, LANES // 2)
        power = tile[:, heads_all - 2 : heads_all - 1]
        scales.append(jnp.exp2(power - UP))
        packed = packed + tile * scales[-1]
        squares = squares + tile[:, heads_all - 1 : heads_all] * jnp.exp2(2.0 * power)

    def total(parts, start):
        value = 0.0
        for part, scale in zip(parts, scales):
            value = value + part[:, start : start + LANES] * scale
        return value

    inv = lax.rsqrt(squares / features + norm_eps)
    log_in = packed[:, :heads] * inv
    raw = packed[:, heads_all : heads_all + heads] * inv + bias[block : block + 1, :]
    log_forget = jnp.minimum(raw, 0.0) - jnp.log1p(jnp.exp(-jnp.abs(raw)))
    mp_s[...] = jnp.zeros(mp_s.shape, F32)
    tall_s[...] = jnp.zeros(tall_s.shape, F32)
    wide_s[...] = jnp.zeros(wide_s.shape, F32)
    wide_s[:heads, :real] = maxval[block]
    tall = wide_s[...].T
    for padded, plain in moves:
        mp_s[padded, :] = tall[plain, :heads]
    carried = log_forget + mp_s[...]
    new_max = jnp.maximum(carried, log_in)
    decays = jnp.exp(carried - new_max)
    weight_in = jnp.exp(log_in - new_max)
    for padded, plain in moves:
        tall_s[plain, :heads] = new_max[padded]
    max_out[...] = tall_s[...].T[:heads, :real]
    part_s[...] = jnp.zeros(part_s.shape, F32)
    for h in range(heads):
        at = h * LANES
        q = total(firsts, at) * inv
        high, rest = pieces(q)
        middle, low = pieces(rest)
        q_t = columns(high, middle, low)
        for row, seq, count in twos(moves):
            spread_q = jnp.dot(
                q_t, ones[:, row * LANES : (row + count) * LANES], preferred_element_type=F32
            )
            for i in range(count):
                product = matrix[seq + i, h] * spread_q[:, i * LANES : (i + 1) * LANES]
                part_s[h, (row + i) * 8 : (row + i) * 8 + 8, :] = jnp.sum(
                    product.reshape(LANES // 8, 8, LANES), axis=0
                )
        v = total(seconds, at) * inv
        v_out[h] = v
        dec = jnp.broadcast_to(decays[:, h : h + 1], (rows, LANES))
        dec_out[h] = dec
        kw = total(firsts, cols + at) * (inv * LANES ** (-0.5)) * weight_in[:, h : h + 1]
        kw_out[h] = kw
        for padded, plain in moves:
            nn = dec[padded] * norm[block, plain, h, :] + kw[padded]
            norm_out[plain, h, :] = nn
            mp_s[padded, h : h + 1] = jnp.sum(q[padded] * nn, axis=1, keepdims=True)
        denominator = jnp.maximum(jnp.abs(mp_s[:, h : h + 1]), 1.0)
        mixed = part_s[h, pl.ds(0, rows, stride=8), :]
        for j in range(1, 8):
            mixed = mixed + part_s[h, pl.ds(j, rows, stride=8), :]
        scores = jnp.sum(q * kw, axis=1, keepdims=True)
        readout = (dec * mixed + scores * v) / denominator
        average = jnp.mean(readout, axis=1, keepdims=True)
        centred = readout - average
        variance = jnp.mean(centred * centred, axis=1, keepdims=True)
        normed = centred * lax.rsqrt(variance + head_eps) * gain[block, h : h + 1, :]
        gate = jax.nn.sigmoid(total(seconds, cols + at) * inv)
        hidden[:, at : at + LANES] = (normed * gate).astype(BF16)


def cell(block, firsts, seconds, bias, gain, norm, maxval, matrix, ones, heads_all, features, earlier, last, after):
    rows = firsts[0].shape[0]
    real, heads = matrix.shape[:2]
    whole = pl.BlockSpec(memory_space=pltpu.VMEM)
    gates = pltpu.VMEM((heads, rows, LANES), F32)
    blocks = block + 1 if last else 1
    earlier = list(earlier) if last else []
    return pl.pallas_call(
        functools.partial(cell_kernel, block, features, heads_all, len(firsts), len(earlier) // 2),
        in_specs=[whole] * (6 + 2 * len(firsts) + len(earlier)) + [pl.BlockSpec(memory_space=pl.ANY)] * len(after),
        out_specs=[whole] * 6,
        out_shape=[
            pltpu.VMEM((rows, heads * LANES), BF16),
            pltpu.VMEM((blocks,) + norm.shape[1:], F32),
            pltpu.VMEM((blocks,) + maxval.shape[1:], F32),
            gates,
            gates,
            gates,
        ],
        scratch_shapes=[
            pltpu.VMEM((rows, heads), F32),
            pltpu.VMEM((heads, rows * 8, LANES), F32),
            pltpu.VMEM((8, LANES), F32),
            pltpu.VMEM((LANES, 8), F32),
        ],
        compiler_params=pltpu.CompilerParams(vmem_limit_bytes=12 << 20),
        cost_estimate=pl.CostEstimate(
            flops=4 * real * heads * LANES * LANES, bytes_accessed=1 << 20, transcendentals=0
        ),
        name="cell",
    )(*firsts, *seconds, bias, gain, norm, maxval, in_vmem(matrix), in_vmem(ones), *earlier, *after)


def update_kernel(block, kw, v, dec, matrix, ones, *rest):
    out, buffer, sems = rest[-3:]
    real, heads = matrix.shape[:2]
    pairs = kw.shape[1] // PAD
    moves = spread(pairs, real // pairs)
    copies = []
    for h in range(heads):
        start = 0
        k_high, k_low = pieces(kw[h])
        k_t = columns(k_high, k_high, k_low)
        v_high, v_low = pieces(v[h])
        v_rows = jnp.concatenate([v_high, v_low, v_high, jnp.zeros_like(v_high)], axis=0).astype(BF16)
        for row, seq, count in twos(moves):
            right = jnp.concatenate(
                [ones[:, (row + i) * LANES : (row + i + 1) * LANES] * v_rows for i in range(count)], axis=1
            )
            outer = jnp.dot(k_t, right, preferred_element_type=F32)
            for i in range(count):
                decay = dec[h, row + i : row + i + 1, :]
                buffer[h, seq + i] = decay * matrix[seq + i, h] + outer[:, i * LANES : (i + 1) * LANES]
            done = seq + count
            if done * STORES % real < count * STORES:
                part = pl.ds(start, done - start)
                copies.append(
                    pltpu.make_async_copy(
                        buffer.at[h, part], out.at[block, part, h], sems.at[len(copies)]
                    )
                )
                copies[-1].start()
                start = done
    for copy in copies:
        copy.wait()


def update(block, blocks, kw, v, dec, matrix, ones, filled):
    real, heads = matrix.shape[:2]
    whole = pl.BlockSpec(memory_space=pltpu.VMEM)
    aliased = [] if filled is None else [filled]
    return pl.pallas_call(
        functools.partial(update_kernel, block),
        in_specs=[whole] * 5 + [pl.BlockSpec(memory_space=pltpu.HBM)] * len(aliased),
        out_specs=pl.BlockSpec(memory_space=pltpu.HBM),
        out_shape=pltpu.HBM((blocks,) + matrix.shape, F32),
        input_output_aliases={5: 0} if aliased else {},
        scratch_shapes=[
            pltpu.VMEM((heads, real, LANES, LANES), F32),
            pltpu.SemaphoreType.DMA((heads * (STORES + 1),)),
        ],
        compiler_params=pltpu.CompilerParams(vmem_limit_bytes=12 << 20),
        cost_estimate=pl.CostEstimate(
            flops=8 * real * heads * LANES * LANES,
            bytes_accessed=4 * real * heads * LANES * LANES,
            transcendentals=0,
        ),
        name="update",
    )(kw, v, dec, in_vmem(matrix), in_vmem(ones), *map(in_hbm, aliased))


def output_kernel(block, slots, w, *refs):
    parts, out = refs[:slots], refs[-1]
    rows = parts[0].shape[0]
    me = lax.axis_index("dp")
    value = jnp.dot(
        jnp.concatenate([part[...] for part in parts], axis=0), w[block], preferred_element_type=F32
    )
    value = value * OUT_UP
    for slot in range(slots):
        start = pl.multiple_of((me ^ slot) * rows, rows)
        out[pl.ds(start, rows), :] = value[slot * rows : (slot + 1) * rows]


def output(block, w, parts, after):
    rows = parts[0].shape[0]
    whole = pl.BlockSpec(memory_space=pltpu.VMEM)
    return pl.pallas_call(
        functools.partial(output_kernel, block, len(parts)),
        in_specs=[whole] * (1 + len(parts)) + [pl.BlockSpec(memory_space=pl.ANY)] * len(after),
        out_specs=whole,
        out_shape=pltpu.VMEM((rows * len(parts), w.shape[2]), F32),
        compiler_params=pltpu.CompilerParams(vmem_limit_bytes=8 << 20),
        cost_estimate=pl.CostEstimate(
            flops=2 * rows * len(parts) * w.shape[1] * w.shape[2], bytes_accessed=1 << 20, transcendentals=0
        ),
        name="output",
    )(in_vmem(w), *parts, *after)


def swap(x, axis, size, bit):
    return lax.ppermute(x, axis, [(i, i ^ bit) for i in range(size)])


def on_device(
    tokens,
    w_query,
    w_key,
    w_value,
    w_outgate,
    w_ingate,
    w_forget,
    forget_bias,
    head_gain,
    w_proj,
    mem_matrix,
    mem_norm,
    mem_max,
):
    tp, dp = lax.axis_size("tp"), lax.axis_size("dp")
    real = tokens.shape[0]
    features = tokens.shape[1]
    heads = forget_bias.shape[1]
    heads_all = w_ingate.shape[2]
    assert dp & (dp - 1) == 0 and tp % dp == 0 and real <= PAD and 2 * heads_all <= LANES // 2
    assert tp // dp * PAD == ROWS and heads < heads_all - 2
    w_ingate, w_forget = w_ingate.swapaxes(1, 2), w_forget.swapaxes(1, 2)
    mem_max = mem_max.swapaxes(1, 2)
    blocks = w_query.shape[0]
    weights, later = (w_query, w_key, w_ingate, w_forget), (w_value, w_outgate)
    copied, *first = begin(tokens, weights, tp)
    current = lax.all_to_all(copied, "tp", 0, 0)
    earlier, matrix_out, after = [], None, ()
    for block in range(blocks):
        if block == 0:
            firsts, seconds = project(block, heads, current, first, later, dp)
        else:
            firsts, seconds = project(block, heads, current, weights + later, (), dp)
        state = [(mem_matrix.shape[1:], F32)]
        if block == 0:
            *matrices, ones = fetch((mem_matrix,), [(0, 0, 0, None)], state, True, (seconds[0],))
            after = tuple(matrices)
        hidden, norm_out, max_out, kw, v, dec = cell(
            block, firsts, seconds, forget_bias, head_gain, mem_norm, mem_max, matrices[block], ones,
            heads_all, features * dp, earlier, block + 1 == blocks, after,
        )
        earlier += [norm_out, max_out]
        gathered = [hidden] + [swap(hidden, "dp", dp, slot) for slot in range(1, dp)]
        matrix_out = update(block, blocks, kw, v, dec, matrices[block], ones, matrix_out)
        after = (in_hbm(matrix_out),)
        fillers = after
        if block + 1 < blocks:
            fillers = fetch((mem_matrix,), [(0, block + 1, 0, None)], state, False, (hidden,))
            matrices += fillers
        partial = output(block, w_proj, gathered, tuple(fillers)).reshape(tp, PAD, features)
        summed = lax.all_to_all(partial.astype(jnp.float16), "tp", 0, 0)
        summed = (jnp.sum(summed.astype(F32), axis=0) * (1.0 / OUT_UP)).astype(BF16)
        if block + 1 < blocks:
            current = lax.all_to_all(jnp.broadcast_to(summed[None], (tp,) + summed.shape), "tp", 0, 0)
    return (summed[:real], matrix_out, norm_out, max_out.swapaxes(1, 2))


def solution(mesh):
    in_specs = (
        P("tp", "dp"),
        P(None, "dp", "tp"),
        P(None, "dp", "tp"),
        P(None, "dp", "tp"),
        P(None, "dp", "tp"),
        P(None, "dp", None),
        P(None, "dp", None),
        P(None, "tp"),
        P(None, "tp", None),
        P(None, "tp", "dp"),
        P(None, "dp", "tp", None, None),
        P(None, "dp", "tp", None),
        P(None, "dp", "tp"),
    )
    out_specs = (
        P("tp", "dp"),
        P(None, "dp", "tp", None, None),
        P(None, "dp", "tp", None),
        P(None, "dp", "tp"),
    )
    return jax.shard_map(
        on_device, mesh=mesh, in_specs=in_specs, out_specs=out_specs, check_vma=False
    )
```

```python
import functools

import jax
import jax.numpy as jnp
from jax import lax
from jax.experimental import pallas as pl
from jax.experimental.pallas import tpu as pltpu
from jax.sharding import PartitionSpec as P


norm_eps = 1e-06
head_eps = 1e-05
ROWS = 32
PAD = 16
LANES = 128
UP = 12.0
TINY = 1e-30
STORES = 4
OUT_UP = 16.0
F32 = jnp.float32
BF16 = jnp.bfloat16


def in_hbm(x):
    return pltpu.with_memory_space_constraint(x, pltpu.HBM)


def in_vmem(x):
    return pltpu.with_memory_space_constraint(x, pltpu.VMEM)


def lane_roll(x, amount):
    return pltpu.roll(x, amount % x.shape[-1], 1)


def begin_kernel(tokens, *refs):
    count = (len(refs) - 3) // 2
    sources, (copied, ones, *targets), sems = refs[:count], refs[count:-1], refs[-1]
    moves = [(tokens, copied.at[i]) for i in range(copied.shape[0])]
    moves += [(source.at[:1], target) for source, target in zip(sources, targets)]
    copies = [
        pltpu.make_async_copy(source, target, sems.at[i]) for i, (source, target) in enumerate(moves)
    ]
    for copy in copies:
        copy.start()
    row = lax.broadcasted_iota(jnp.int32, (LANES, LANES), 0)
    for block in range(ROWS):
        here = (row % ROWS == block) & (row < 3 * ROWS)
        ones[:, block * LANES : (block + 1) * LANES] = jnp.where(here, 1.0, 0.0).astype(BF16)
    for copy in copies:
        copy.wait()


def begin(tokens, weights, copies):
    shapes = [((copies,) + tokens.shape, BF16), ((LANES, ROWS * LANES), BF16)] + [((1,) + w.shape[1:], BF16) for w in weights]
    whole = pl.BlockSpec(memory_space=pltpu.VMEM)
    return pl.pallas_call(
        begin_kernel,
        in_specs=[pl.BlockSpec(memory_space=pltpu.HBM)] * (1 + len(weights)),
        out_specs=[whole] * len(shapes),
        out_shape=[pltpu.VMEM(shape, dtype) for shape, dtype in shapes],
        scratch_shapes=[pltpu.SemaphoreType.DMA((copies + len(weights),))],
        compiler_params=pltpu.CompilerParams(vmem_limit_bytes=8 << 20),
        cost_estimate=pl.CostEstimate(flops=1 << 36, bytes_accessed=1 << 27, transcendentals=0),
        name="begin",
    )(*map(in_hbm, (tokens,) + weights))


def first_project_kernel(block, heads_all, heads, x, wq, wk, wi, wf, *rest):
    later = (len(rest) - 5) // 2
    keep, send, x_rel, gates = rest[later : later + 3] + (rest[2 * later + 3],)
    copies = []
    for source, target in zip(rest[:later], rest[later + 3 : 2 * later + 3]):
        copies.append(pltpu.make_async_copy(source.at[:1], target, rest[-1].at[len(copies)]))
        copies[-1].start()
    rows = ROWS
    slots = x_rel.shape[0] // rows
    me = lax.axis_index("dp")
    first_head = lax.axis_index("tp") * heads
    pairs, real = rows // PAD, x.shape[1]
    if real < PAD:
        x_rel[...] = jnp.zeros(x_rel.shape, BF16)
    for place, slot in enumerate(slot_order(slots)):
        for i in range(pairs):
            at = place * rows + i * PAD
            x_rel[at : at + real, :] = x[(me ^ slot) * pairs + i]
    xs = x_rel[...]
    cols = wq.shape[2]
    half = keep.shape[0]

    def emit(value, offset):
        width = value.shape[1]
        keep[:, offset : offset + width] = value[:half]
        send[:, offset : offset + width] = value[half:]

    for index, weight in enumerate((wq, wk)):
        emit(jnp.dot(xs, weight[block], preferred_element_type=F32), index * cols)
    wide = xs.astype(F32)
    squares = jnp.sum(wide * wide, axis=1, keepdims=True)
    gates[...] = jnp.zeros(gates.shape, F32)
    for index, weight in enumerate((wi, wf)):
        value = lax.dot_general(xs, weight[block], (((1,), (1,)), ((), ())), preferred_element_type=F32)
        gates[:, index * heads_all : (index + 1) * heads_all] = value
    lane = lax.broadcasted_iota(jnp.int32, gates.shape, 1)
    mine = pltpu.roll(gates[...], (LANES - first_head) % LANES, 1)
    emit(jnp.where(lane == heads_all - 1, squares, mine), 2 * cols)
    for copy in copies:
        copy.wait()


def second_project_kernel(block, x_rel, wv, wo, keep, send):
    xs = x_rel[...]
    cols = wv.shape[2]
    half = keep.shape[0]
    for index, weight in enumerate((wv, wo)):
        value = jnp.dot(xs, weight[block], preferred_element_type=F32)
        keep[:, index * cols : (index + 1) * cols] = value[:half]
        send[:, index * cols : (index + 1) * cols] = value[half:]


def first_add_kernel(heads_all, keep, other, scale_out, *outs):
    wide = keep.shape[1]
    tile = keep[:, wide - LANES :] + other[:, wide - LANES :]
    squares = tile[:, heads_all - 1 : heads_all]
    power = jnp.floor(0.5 * jnp.log2(squares + TINY))
    scale = jnp.exp2(UP - power)
    scale_out[...] = jnp.broadcast_to(scale, scale_out.shape)
    lane = lax.broadcasted_iota(jnp.int32, tile.shape, 1)
    tile = tile * scale
    tile = jnp.where(lane == heads_all - 1, squares * jnp.exp2(-2.0 * power), tile)
    tile = jnp.where(lane == heads_all - 2, power, tile)
    low = tile - tile.astype(BF16).astype(F32)
    tile = jnp.where(lane < LANES // 2, tile, pltpu.roll(low, LANES // 2, 1))
    for i, out in enumerate(outs):
        at = slice(i * ROWS, (i + 1) * ROWS)
        out[:, : wide - LANES] = (keep[at, : wide - LANES] + other[at, : wide - LANES]) * scale[at]
        out[:, wide - LANES :] = tile[at]


def second_add_kernel(keep, other, scale, *outs):
    for i, out in enumerate(outs):
        at = slice(i * ROWS, (i + 1) * ROWS)
        out[...] = (keep[at] + other[at]) * scale[at, :1]


def slot_order(slots):
    return list(range(0, slots, 2)) + list(range(1, slots, 2))


def small_call(kernel, shapes, args, scratch=(), in_place=0, flops=0):
    whole = pl.BlockSpec(memory_space=pltpu.VMEM)
    return pl.pallas_call(
        kernel,
        in_specs=[whole] * (len(args) - in_place) + [pl.BlockSpec(memory_space=pltpu.HBM)] * in_place,
        out_specs=[whole] * len(shapes),
        out_shape=[pltpu.VMEM(shape, dtype) for shape, dtype in shapes],
        scratch_shapes=list(scratch),
        compiler_params=pltpu.CompilerParams(vmem_limit_bytes=8 << 20),
        cost_estimate=pl.CostEstimate(flops=flops, bytes_accessed=1 << 20, transcendentals=0),
    )(*args)


def without(kernel, start, count):
    return lambda *refs: kernel(*refs[:start], *refs[start + count :])


def project(block, heads, x, weights, later, slots, ahead=()):
    wq, wk, wi, wf, *others = map(in_vmem, weights)
    later = [in_hbm(w) for w in later]
    all_rows, features = slots * ROWS, x.shape[2]
    half = all_rows // 2
    cols, heads_all = wq.shape[2], wi.shape[1]
    first, second = 2 * cols + LANES, 2 * cols
    flops = 2 * all_rows * features * second
    scratch = [pltpu.VMEM((all_rows, LANES), F32), pltpu.SemaphoreType.DMA((max(len(later), 1),))]
    keep_a, send_a, x_rel, *fetched = small_call(
        without(functools.partial(first_project_kernel, block, heads_all, heads), 5, len(ahead)),
        [((half, first), F32)] * 2
        + [((all_rows, features), BF16)]
        + [((1,) + w.shape[1:], BF16) for w in later],
        (x, wq, wk, wi, wf, *map(in_vmem, ahead), *later),
        scratch,
        len(later),
        flops,
    )
    wv, wo = fetched or others
    other_a = swap(send_a, "dp", slots, 1)
    keep_b, send_b = small_call(
        functools.partial(second_project_kernel, block), [((half, second), F32)] * 2, (x_rel, wv, wo), flops=flops
    )
    other_b = swap(send_b, "dp", slots, 1)
    scale, *sums_a = small_call(
        functools.partial(first_add_kernel, heads_all),
        [((half, LANES), F32)] + [((ROWS, first), F32)] * (slots // 2),
        (keep_a, other_a),
        flops=1 << 20,
    )
    sums_b = small_call(
        second_add_kernel, [((ROWS, second), F32)] * (slots // 2), (keep_b, other_b, scale), flops=1 << 20
    )

    def across(sums):
        return [sums[0]] + [
            swap(part.astype(jnp.float16), "dp", slots, slot).astype(F32)
            for part, slot in zip(sums[1:], range(2, slots, 2))
        ]

    firsts = across(sums_a)
    return firsts, across(sums_b)


def spread(pairs, real):
    return [(slice(i * PAD, i * PAD + real), slice(i * real, (i + 1) * real)) for i in range(pairs)]


def twos(moves):
    runs = []
    for padded, plain in moves:
        length = plain.stop - plain.start
        for j in range(0, length, 2):
            runs.append((padded.start + j, plain.start + j, min(2, length - j)))
    return runs


def pieces(x):
    high = x.astype(BF16).astype(F32)
    return high, x - high


def columns(*parts):
    parts = list(parts)
    rest = LANES - sum(part.shape[0] for part in parts)
    if rest:
        parts.append(jnp.zeros((rest, LANES), F32))
    return jnp.concatenate(parts, axis=0).T.astype(BF16)


def read_kernel(block, features, heads_all, peers, before, *refs):
    firsts = refs[:peers]
    bias, norm, maxval, matrix, ones = refs[peers : peers + 5]
    earlier = refs[peers + 5 : peers + 5 + 2 * before]
    (base, weight, scale_out, norm_out, max_out, kw_out, dec_out, mp_s, part_s, wide_s, tall_s) = refs[-11:]
    real, heads = matrix.shape[1:3]
    rows = base.shape[1]
    pairs = rows // PAD
    moves = spread(pairs, real // pairs)
    cols = heads * LANES

    for i in range(before):
        norm_out[i] = earlier[2 * i][0]
        max_out[i] = earlier[2 * i + 1][0]
    norm_out, max_out = norm_out.at[before], max_out.at[before]

    scales, packed, squares = [], 0.0, 0.0
    for part in firsts:
        tile = part[:, 2 * cols :]
        tile = tile + lane_roll(tile, LANES // 2)
        power = tile[:, heads_all - 2 : heads_all - 1]
        scales.append(jnp.exp2(power - UP))
        packed = packed + tile * scales[-1]
        squares = squares + tile[:, heads_all - 1 : heads_all] * jnp.exp2(2.0 * power)

    def total(parts, start):
        value = 0.0
        for part, scale in zip(parts, scales):
            value = value + part[:, start : start + LANES] * scale
        return value

    inv = lax.rsqrt(squares / features + norm_eps)
    for i, scale in enumerate(scales):
        scale_out[i] = jnp.broadcast_to(scale * inv, (rows, LANES))
    log_in = packed[:, :heads] * inv
    raw = packed[:, heads_all : heads_all + heads] * inv + bias[block : block + 1, :]
    log_forget = jnp.minimum(raw, 0.0) - jnp.log1p(jnp.exp(-jnp.abs(raw)))
    mp_s[...] = jnp.zeros(mp_s.shape, F32)
    tall_s[...] = jnp.zeros(tall_s.shape, F32)
    wide_s[...] = jnp.zeros(wide_s.shape, F32)
    wide_s[:heads, :real] = maxval[block]
    tall = wide_s[...].T
    for padded, plain in moves:
        mp_s[padded, :] = tall[plain, :heads]
    carried = log_forget + mp_s[...]
    new_max = jnp.maximum(carried, log_in)
    decays = jnp.exp(carried - new_max)
    weight_in = jnp.exp(log_in - new_max)
    for padded, plain in moves:
        tall_s[plain, :heads] = new_max[padded]
    max_out[...] = tall_s[...].T[:heads, :real]
    part_s[...] = jnp.zeros(part_s.shape, F32)
    for h in range(heads):
        at = h * LANES
        q = total(firsts, at) * inv
        high, rest = pieces(q)
        middle, low = pieces(rest)
        q_t = columns(high, middle, low)
        for row, seq, count in twos(moves):
            spread_q = jnp.dot(
                q_t, ones[:, row * LANES : (row + count) * LANES], preferred_element_type=F32
            )
            for i in range(count):
                product = matrix[block, seq + i, h] * spread_q[:, i * LANES : (i + 1) * LANES]
                part_s[h, (row + i) * 8 : (row + i) * 8 + 8, :] = jnp.sum(
                    product.reshape(LANES // 8, 8, LANES), axis=0
                )
        dec = jnp.broadcast_to(decays[:, h : h + 1], (rows, LANES))
        dec_out[h] = dec
        kw = total(firsts, cols + at) * (inv * LANES ** (-0.5)) * weight_in[:, h : h + 1]
        kw_out[h] = kw
        for padded, plain in moves:
            nn = dec[padded] * norm[block, plain, h, :] + kw[padded]
            norm_out[plain, h, :] = nn
            mp_s[padded, h : h + 1] = jnp.sum(q[padded] * nn, axis=1, keepdims=True)
        denominator = jnp.maximum(jnp.abs(mp_s[:, h : h + 1]), 1.0)
        mixed = part_s[h, pl.ds(0, rows, stride=8), :]
        for j in range(1, 8):
            mixed = mixed + part_s[h, pl.ds(j, rows, stride=8), :]
        scores = jnp.sum(q * kw, axis=1, keepdims=True)
        base[h] = dec * mixed / denominator
        weight[h] = jnp.broadcast_to(scores / denominator, (rows, LANES))


def write_kernel(block, peers, *refs):
    seconds = refs[:peers]
    base, weight, scale, gain, hidden, v_out = refs[peers : peers + 6]
    heads = base.shape[0]
    cols = heads * LANES

    def total(start):
        value = 0.0
        for i, part in enumerate(seconds):
            value = value + part[:, start : start + LANES] * scale[i]
        return value

    for h in range(heads):
        at = h * LANES
        v = total(at)
        v_out[h] = v
        readout = base[h] + weight[h] * v
        average = jnp.mean(readout, axis=1, keepdims=True)
        centred = readout - average
        variance = jnp.mean(centred * centred, axis=1, keepdims=True)
        normed = centred * lax.rsqrt(variance + head_eps) * gain[block, h : h + 1, :]
        gate = jax.nn.sigmoid(total(cols + at))
        hidden[:, at : at + LANES] = (normed * gate).astype(BF16)


def read(block, firsts, bias, norm, maxval, matrix, ones, heads_all, features, earlier, last, after):
    rows = firsts[0].shape[0]
    real, heads = matrix.shape[1:3]
    whole = pl.BlockSpec(memory_space=pltpu.VMEM)
    gates = pltpu.VMEM((heads, rows, LANES), F32)
    blocks = block + 1 if last else 1
    earlier = list(earlier) if last else []
    return pl.pallas_call(
        functools.partial(read_kernel, block, features, heads_all, len(firsts), len(earlier) // 2),
        in_specs=[whole] * (5 + len(firsts) + len(earlier)) + [pl.BlockSpec(memory_space=pl.ANY)] * len(after),
        out_specs=[whole] * 7,
        out_shape=[
            gates,
            gates,
            pltpu.VMEM((len(firsts), rows, LANES), F32),
            pltpu.VMEM((blocks,) + norm.shape[1:], F32),
            pltpu.VMEM((blocks,) + maxval.shape[1:], F32),
            gates,
            gates,
        ],
        scratch_shapes=[
            pltpu.VMEM((rows, heads), F32),
            pltpu.VMEM((heads, rows * 8, LANES), F32),
            pltpu.VMEM((8, LANES), F32),
            pltpu.VMEM((LANES, 8), F32),
        ],
        compiler_params=pltpu.CompilerParams(vmem_limit_bytes=12 << 20),
        cost_estimate=pl.CostEstimate(
            flops=4 * real * heads * LANES * LANES, bytes_accessed=1 << 20, transcendentals=0
        ),
        name="read",
    )(*firsts, bias, norm, maxval, in_vmem(matrix), in_vmem(ones), *earlier, *after)


def write(block, seconds, base, weight, scale, gain):
    heads, rows, _ = base.shape
    return small_call(
        functools.partial(write_kernel, block, len(seconds)),
        [((rows, heads * LANES), BF16), (base.shape, F32)],
        (*seconds, base, weight, scale, gain),
        flops=1 << 20,
    )


def update_kernel(block, span, stored, kw, v, dec, matrix, ones, *rest):
    small, outs, (buffer, sems) = rest[:stored], rest[-3 - stored : -2], rest[-2:]
    out = outs[0]
    real, _ = matrix.shape[1:3]
    pairs = kw.shape[1] // PAD
    moves = spread(pairs, real // pairs)
    copies = []
    for source, target in zip(small, outs[1:]):
        copies.append(pltpu.make_async_copy(source, target, sems.at[len(copies)]))
        copies[-1].start()
    for h in range(*span):
        start = 0
        k_high, k_low = pieces(kw[h])
        k_t = columns(k_high, k_high, k_low)
        v_high, v_low = pieces(v[h])
        v_rows = jnp.concatenate([v_high, v_low, v_high, jnp.zeros_like(v_high)], axis=0).astype(BF16)
        for row, seq, count in twos(moves):
            right = jnp.concatenate(
                [ones[:, (row + i) * LANES : (row + i + 1) * LANES] * v_rows for i in range(count)], axis=1
            )
            outer = jnp.dot(k_t, right, preferred_element_type=F32)
            for i in range(count):
                decay = dec[h, row + i : row + i + 1, :]
                buffer[h - span[0], seq + i] = decay * matrix[block, seq + i, h] + outer[:, i * LANES : (i + 1) * LANES]
            done = seq + count
            if done * STORES % real < count * STORES:
                part = pl.ds(start, done - start)
                copies.append(
                    pltpu.make_async_copy(
                        buffer.at[h - span[0], part], out.at[block, part, h], sems.at[len(copies)]
                    )
                )
                copies[-1].start()
                start = done
    for copy in copies:
        copy.wait()


def update(block, span, kw, v, dec, matrix, ones, filled, small):
    real, heads = matrix.shape[1:3]
    whole = pl.BlockSpec(memory_space=pltpu.VMEM)
    aliased = [] if filled is None else [filled]
    return pl.pallas_call(
        functools.partial(update_kernel, block, span, len(small)),
        in_specs=[whole] * (5 + len(small)) + [pl.BlockSpec(memory_space=pltpu.HBM)] * len(aliased),
        out_specs=[pl.BlockSpec(memory_space=pltpu.HBM)] * (1 + len(small)),
        out_shape=[pltpu.HBM(matrix.shape, F32)] + [pltpu.HBM(a.shape, F32) for a in small],
        input_output_aliases={5 + len(small): 0} if aliased else {},
        scratch_shapes=[
            pltpu.VMEM((span[1] - span[0], real, LANES, LANES), F32),
            pltpu.SemaphoreType.DMA((heads * (STORES + 1) + len(small),)),
        ],
        compiler_params=pltpu.CompilerParams(vmem_limit_bytes=12 << 20),
        cost_estimate=pl.CostEstimate(
            flops=8 * real * (span[1] - span[0]) * LANES * LANES,
            bytes_accessed=4 * real * heads * LANES * LANES,
            transcendentals=0,
        ),
        name="update",
    )(kw, v, dec, in_vmem(matrix), in_vmem(ones), *map(in_vmem, small), *map(in_hbm, aliased))


def output_kernel(block, slots, w, *refs):
    parts, out = refs[:slots], refs[-1]
    rows = parts[0].shape[0]
    me = lax.axis_index("dp")
    value = jnp.dot(
        jnp.concatenate([part[...] for part in parts], axis=0), w[block], preferred_element_type=F32
    )
    value = value * OUT_UP
    for slot in range(slots):
        start = pl.multiple_of((me ^ slot) * rows, rows)
        out[pl.ds(start, rows), :] = value[slot * rows : (slot + 1) * rows]


def output(block, w, parts, after):
    rows = parts[0].shape[0]
    whole = pl.BlockSpec(memory_space=pltpu.VMEM)
    return pl.pallas_call(
        functools.partial(output_kernel, block, len(parts)),
        in_specs=[whole] * (1 + len(parts)) + [pl.BlockSpec(memory_space=pl.ANY)] * len(after),
        out_specs=whole,
        out_shape=pltpu.VMEM((rows * len(parts), w.shape[2]), F32),
        compiler_params=pltpu.CompilerParams(vmem_limit_bytes=8 << 20),
        cost_estimate=pl.CostEstimate(
            flops=2 * rows * len(parts) * w.shape[1] * w.shape[2], bytes_accessed=1 << 20, transcendentals=0
        ),
        name="output",
    )(in_vmem(w), *parts, *after)


def swap(x, axis, size, bit):
    return lax.ppermute(x, axis, [(i, i ^ bit) for i in range(size)])


def on_device(
    tokens,
    w_query,
    w_key,
    w_value,
    w_outgate,
    w_ingate,
    w_forget,
    forget_bias,
    head_gain,
    w_proj,
    mem_matrix,
    mem_norm,
    mem_max,
):
    tp, dp = lax.axis_size("tp"), lax.axis_size("dp")
    real = tokens.shape[0]
    features = tokens.shape[1]
    heads = forget_bias.shape[1]
    heads_all = w_ingate.shape[2]
    assert dp & (dp - 1) == 0 and tp % dp == 0 and real <= PAD and 2 * heads_all <= LANES // 2
    assert tp // dp * PAD == ROWS and heads < heads_all - 2
    w_ingate, w_forget = w_ingate.swapaxes(1, 2), w_forget.swapaxes(1, 2)
    mem_max = mem_max.swapaxes(1, 2)
    blocks = w_query.shape[0]
    weights, later = (w_query, w_key, w_ingate, w_forget), (w_value, w_outgate)
    copied, ones = begin(tokens, (), tp)
    current = lax.all_to_all(copied, "tp", 0, 0)
    earlier, matrix_out, after, held = [], None, (), None
    for block in range(blocks):
        firsts, seconds = project(block, heads, current, weights + later, (), dp, later)
        last = block + 1 == blocks
        if held:
            matrix_out, *_ = update(block - 1, *held, mem_matrix, ones, matrix_out, ())
            after = (in_hbm(matrix_out),)
        base, weight, scale, norm_out, max_out, kw, dec = read(
            block, firsts, forget_bias, mem_norm, mem_max, mem_matrix, ones,
            heads_all, features * dp, earlier, last, after,
        )
        hidden, v = write(block, seconds, base, weight, scale, head_gain)
        earlier += [norm_out, max_out]
        gathered = [hidden] + [swap(hidden, "dp", dp, slot) for slot in range(1, dp)]
        split = heads if last else (heads + 3) // 4
        small = (norm_out, max_out) if last else ()
        matrix_out, *stored = update(block, (0, split), kw, v, dec, mem_matrix, ones, matrix_out, small)
        held = ((split, heads), kw, v, dec) if split < heads else None
        after = (in_hbm(matrix_out),)
        partial = output(block, w_proj, gathered, after).reshape(tp, PAD, features)
        summed = lax.all_to_all(partial.astype(jnp.float16), "tp", 0, 0)
        summed = (jnp.sum(summed.astype(F32), axis=0) * (1.0 / OUT_UP)).astype(BF16)
        if block + 1 < blocks:
            current = lax.all_to_all(jnp.broadcast_to(summed[None], (tp,) + summed.shape), "tp", 0, 0)
    return (summed[:real], matrix_out, stored[0], stored[1].swapaxes(1, 2))


def solution(mesh):
    in_specs = (
        P("tp", "dp"),
        P(None, "dp", "tp"),
        P(None, "dp", "tp"),
        P(None, "dp", "tp"),
        P(None, "dp", "tp"),
        P(None, "dp", None),
        P(None, "dp", None),
        P(None, "tp"),
        P(None, "tp", None),
        P(None, "tp", "dp"),
        P(None, "dp", "tp", None, None),
        P(None, "dp", "tp", None),
        P(None, "dp", "tp"),
    )
    out_specs = (
        P("tp", "dp"),
        P(None, "dp", "tp", None, None),
        P(None, "dp", "tp", None),
        P(None, "dp", "tp"),
    )
    return jax.shard_map(
        on_device, mesh=mesh, in_specs=in_specs, out_specs=out_specs, check_vma=False
    )
```
